512 devices in a mesh: ep: 128 (over z, x, core), tp: 4 (over y).
Axes of the slice: x: 4, y: 4, z: 16, core: 2. Of those that a mesh axis runs over, the one named last changes fastest.
Arguments:
- hidden_in: bfloat16 [2048, 1024], P('ep'), may hold values from -6 to 6
- attn_gain: float32 [1024], replicated, may hold values from 0.1 to 1.9
- w_qdown: bfloat16 [1024, 256], replicated, may hold values from -0.1875 to 0.1875
- q_gain: float32 [256], replicated, may hold values from 0.1 to 1.9
- w_qnope: bfloat16 [256, 512], replicated, may hold values from -0.375 to 0.375
- w_qrope: bfloat16 [256, 256], replicated, may hold values from -0.375 to 0.375
- w_kvdown: bfloat16 [1024, 128], replicated, may hold values from -0.1875 to 0.1875
- kv_gain: float32 [128], replicated, may hold values from 0.1 to 1.9
- w_krope: bfloat16 [1024, 32], replicated, may hold values from -0.1875 to 0.1875
- w_ukey: bfloat16 [128, 512], replicated, may hold values from -0.75 to 0.75
- w_uvalue: bfloat16 [128, 512], replicated, may hold values from -0.5 to 0.5
- w_out: bfloat16 [512, 1024], P('tp'), may hold values from -0.25 to 0.25
- cache_latent: bfloat16 [2048, 1024, 128], P(('ep', 'tp')), may hold values from -6 to 6
- cache_rope: bfloat16 [2048, 32, 1024], P(('ep', 'tp')), may hold values from -900 to 900
- lengths: int32 [2048], P(('ep', 'tp')), may hold values from 1 to 1024, as said below
- ffn_gain: float32 [1024], replicated, may hold values from 0.1 to 1.9
- routes: int32 [2048, 2], P('ep'), may hold values from 0 to 63, all different within a row; in each aligned block of 16 rows (0 to 15, 16 to 31, ...) at most 2 rows name the same one
- route_weights: float32 [2048, 2], P('ep'), may hold values from 0.25 to 1
- w_gate: bfloat16 [128, 1024, 1792], P('ep', None, 'tp'), may hold values from -0.1875 to 0.1875
- w_up: bfloat16 [128, 1024, 1792], P('ep', None, 'tp'), may hold values from -0.1875 to 0.1875
- w_down: bfloat16 [128, 1792, 1024], P('ep', 'tp'), may hold values from -0.09375 to 0.09375
Outputs:
- next_hidden: bfloat16 [2048, 1024], P('ep', 'tp')
The draws below stay inside these ranges and needn't reach their ends.
Inputs may be any that keep to these rules, and one draw needn't show every extreme that they name: `lengths`: each sequence has 1 to 1024 valid cached positions; in every aligned block of 16 sequences one has all 1024. `routes`: each row names two different experts. In the aligned blocks of 16 rows no expert is named by more than 2 rows, and in some block one expert is named by exactly 2.
All inputs are finite; a program needn't handle non-finite values.
Results may differ from the reference program's by a relative error of at most 0.014.
The reference program's roundings to bfloat16 on the way count: a program that leaves them out, or rounds other values in their place, can miss the bound.
Values may be sent and summed in bfloat16 or wider, within the bound.
No kernel may reach another device: no remote copies, remote signals or barrier semaphores. Data moves between devices by JAX's collectives and lax.ppermute only.
A program may use at most 64 MiB of HBM per device.

```python
import math
import jax
import jax.numpy as jnp
import numpy as np
from jax import lax

D = 1024
HEADS = 8
NOPE = 64
ROPE = 32
VDIM = 64
QLORA = 256
KVLORA = 128
EXPERT_FF = 3584
CACHE = 1024
FF_HALF = 1792
SEQ_GRP = 16
TOKENS = 2048
EXPERTS = 64
UNITS = 128
CAP = 2
N_EP = 128
N_TP = 4


def draw_lengths(key, part):
    key_set = jax.random.split(key, 4)
    longer = jax.random.randint(key_set[0], (TOKENS,), 1, CACHE + 1)
    shorter = jax.random.randint(key_set[1], (TOKENS,), 1, 9)
    chosen_short = jax.random.randint(key_set[2], (TOKENS,), 0, 2) == 0
    merged = jnp.where(chosen_short, shorter, longer).reshape(TOKENS // SEQ_GRP, SEQ_GRP)
    full_slot = jax.random.randint(key_set[3], (TOKENS // SEQ_GRP, 1), 0, SEQ_GRP)
    marked = jnp.arange(SEQ_GRP)[None, :] == full_slot
    return jnp.where(marked, CACHE, merged).reshape(TOKENS).astype(jnp.int32)


def draw_cache_rope(key, part):
    key_pair = jax.random.split(key, 1)
    values = jnp.clip(jax.random.normal(key_pair[0], (TOKENS, ROPE, CACHE), jnp.float32), -6.0, 6.0)
    return values.astype(jnp.bfloat16)


def steps_of(rng, dims, shards, least, largest):
    factor_of = 1.0
    for position, blocks in shards:
        heights = jax.random.uniform(jax.random.fold_in(jax.random.fold_in(rng, 6), position), (blocks,), jnp.float32, least / len(shards), largest / len(shards))
        factor_of = factor_of * jnp.repeat(jnp.exp(heights), dims[position] // blocks).reshape((-1,) + (1,) * (len(dims) - 1 - position))
    return factor_of


def assign_block(key, own, number, rows, amount, top, most, skew):
    sequence = jax.random.permutation(key, amount)
    packed, common = load_shares(amount, rows * top, most, skew, True), load_shares(amount, rows * top, most, skew, False)
    places = jnp.arange(amount)

    def named(sizes, rotation):
        used = int((sizes > 0).sum())
        fixed = max(1, used // 4)
        moved = fixed + (places - fixed + rotation * (used - fixed)) % max(1, amount - fixed)
        return jnp.zeros((amount,), jnp.int32).at[sequence[jnp.where(places < fixed, places, moved)]].set(jnp.asarray(sizes, jnp.int32))

    sizes = jnp.where(number % 4 == 0, named(packed, number // 4), named(common, number - number // 4 - 1))
    mixed = jax.random.permutation(jax.random.fold_in(own, 3), amount)
    giver, taker = mixed[0:amount // 2 * 2:2], mixed[1:amount // 2 * 2:2]
    slack = jnp.minimum(sizes[giver] - 1, most - sizes[taker]) // 2
    slack = jnp.where((giver == sequence[0]) | (taker == sequence[0]) | (sizes[taker] == 0), 0, jnp.maximum(slack, 0))
    moved = jax.random.randint(jax.random.fold_in(own, 4), (amount // 2,), 0, 1 << 20) % (slack + 1)
    sizes = sizes.at[giver].add(-moved).at[taker].add(moved)
    members = jnp.searchsorted(jnp.cumsum(sizes), jnp.arange(rows * top), side="right").astype(jnp.int32)
    grid = members.reshape(top, rows).T
    grid = grid[jax.random.permutation(jax.random.fold_in(own, 1), rows)]
    rotation = jax.random.randint(jax.random.fold_in(own, 2), (rows, 1), 0, top)
    return jnp.take_along_axis(grid, (jnp.arange(top)[None, :] + rotation) % top, axis=1)


def load_shares(count, total, limit, slope, full):
    weights = [(1 << 20) // math.isqrt(grade ** slope) + 1 for grade in range(1, count + 1)]
    largest = limit if full else min(limit, max(-(-total // count), total * weights[0] // sum(weights)))
    least = 1 if total - largest >= count - 1 else 0
    counts, rest = [largest] + [least] * (count - 1), total - largest - least * (count - 1)
    while rest > 0:
        movable = [i for i in range(1, count) if counts[i] < largest] or [i for i in range(1, count) if counts[i] < limit]
        mass, left = sum([weights[i] for i in movable]), rest
        for i in movable:
            addition = min(limit - counts[i], max(1, left * weights[i] // mass), rest)
            counts[i] = counts[i] + addition
            rest = rest - addition
    return np.array(counts)


def gaussian(own_key, extent, deviation, reach, shards=(), kind=jnp.bfloat16):
    level = steps_of(own_key, extent, shards, -0.22, 0.18) if shards else 1.0
    array = jax.random.normal(own_key, extent, jnp.float32) * deviation * level
    return jnp.minimum(jnp.maximum(array, -reach), reach).astype(kind)


def setup_inputs(seed: int = 0) -> dict:
    key_list = jax.random.split(jax.random.key(seed), 22)
    hidden_in = gaussian(key_list[0], (TOKENS, D), 1.0, 6.0, ((0, 128),))
    attn_gain = jnp.clip(1.0 + 0.18 * jax.random.normal(key_list[1], (D,), jnp.float32), 0.1, 1.9)
    w_qdown = gaussian(key_list[2], (D, QLORA), D ** -0.5, 0.1875)
    q_gain = jnp.clip(1.0 + 0.18 * jax.random.normal(key_list[3], (QLORA,), jnp.float32), 0.1, 1.9)
    w_qnope = gaussian(key_list[4], (QLORA, HEADS * NOPE), QLORA ** -0.5, 0.375)
    w_qrope = gaussian(key_list[5], (QLORA, HEADS * ROPE), QLORA ** -0.5, 0.375)
    w_kvdown = gaussian(key_list[6], (D, KVLORA), D ** -0.5, 0.1875)
    kv_gain = jnp.clip(1.0 + 0.18 * jax.random.normal(key_list[7], (KVLORA,), jnp.float32), 0.1, 1.9)
    w_krope = gaussian(key_list[8], (D, ROPE), D ** -0.5, 0.1875)
    w_ukey = gaussian(key_list[9], (KVLORA, HEADS * NOPE), NOPE ** -0.5, 0.75)
    w_uvalue = gaussian(key_list[10], (KVLORA, HEADS * VDIM), KVLORA ** -0.5, 0.5)
    w_out = gaussian(key_list[11], (HEADS * VDIM, D), (HEADS * VDIM) ** -0.5, 0.25, ((0, 4),))
    cache_latent = gaussian(key_list[12], (TOKENS, CACHE, KVLORA), 1.0, 6.0, ((0, 512),))
    cache_rope = draw_cache_rope(jax.random.fold_in(key_list[21], 71), 0)
    lengths = draw_lengths(jax.random.fold_in(key_list[21], 71), 0)
    ffn_gain = jnp.clip(1.0 + 0.18 * jax.random.normal(key_list[15], (D,), jnp.float32), 0.1, 1.9)
    routes_keys = jax.random.split(jax.random.fold_in(key_list[16], 1), TOKENS // SEQ_GRP)
    routes_turns = jax.random.permutation(jax.random.fold_in(key_list[16], 3), TOKENS // SEQ_GRP)
    routes = jax.vmap(lambda own, number: assign_block(jax.random.fold_in(key_list[16], 2), own, number, SEQ_GRP, EXPERTS, 2, CAP, 2))(routes_keys, routes_turns).reshape((TOKENS, 2))
    route_weights = jnp.clip(0.25 + 0.75 * jax.random.uniform(key_list[17], (TOKENS, 2), jnp.float32) ** steps_of(key_list[17], (TOKENS, 2), ((0, 128),), -0.2, 0.2), 0.25, 1.0)
    w_gate = gaussian(key_list[18], (UNITS, D, FF_HALF), D ** -0.5, 0.1875, ((0, 128), (2, 4)))
    w_up = gaussian(key_list[19], (UNITS, D, FF_HALF), D ** -0.5, 0.1875, ((0, 128), (2, 4)))
    w_down = gaussian(key_list[20], (UNITS, FF_HALF, D), EXPERT_FF ** -0.5, 0.09375, ((0, 128), (1, 4)))
    return dict(hidden_in=hidden_in, attn_gain=attn_gain, w_qdown=w_qdown, q_gain=q_gain, w_qnope=w_qnope, w_qrope=w_qrope, w_kvdown=w_kvdown, kv_gain=kv_gain, w_krope=w_krope, w_ukey=w_ukey, w_uvalue=w_uvalue, w_out=w_out, cache_latent=cache_latent, cache_rope=cache_rope, lengths=lengths, ffn_gain=ffn_gain, routes=routes, route_weights=route_weights, w_gate=w_gate, w_up=w_up, w_down=w_down)


eps = 1e-06
rope_base = 10000.0

def rms_scale(values, gain):
    return values * lax.rsqrt(lax.optimization_barrier(jnp.mean(values * values, axis=-1, keepdims=True)) + eps) * gain

def rotate(values, positions):
    width = values.shape[-1]
    middle = width // 2
    inverse = jnp.power(rope_base, -jnp.arange(0, width, 2).astype(jnp.float32) / width)
    angles = positions.astype(jnp.float32)[:, None] * inverse[None, :]
    angles = jnp.concatenate([angles, angles], axis=-1)
    target = (angles.shape[0],) + (1,) * (values.ndim - 2) + (width,)
    cosine = jnp.cos(angles).reshape(target)
    sine = jnp.sin(angles).reshape(target)
    turned = jnp.concatenate([-values[..., middle:], values[..., :middle]], axis=-1)
    return values * cosine + turned * sine

def route_slots(route_table, expert_count):
    flat_ids = route_table.reshape(-1)
    onehot = (flat_ids[:, None] == jnp.arange(expert_count, dtype=jnp.int32)[None, :]).astype(jnp.int32)
    before = jnp.cumsum(onehot, axis=0) - onehot
    return lax.optimization_barrier(jnp.sum(before * onehot, axis=1)).reshape(route_table.shape).astype(jnp.int32)

def reference(hidden_in, attn_gain, w_qdown, q_gain, w_qnope, w_qrope, w_kvdown, kv_gain, w_krope, w_ukey, w_uvalue, w_out, cache_latent, cache_rope, lengths, ffn_gain, routes, route_weights, w_gate, w_up, w_down):
    score_scale = (NOPE + ROPE) ** (-0.5)
    head_block = HEADS * VDIM // N_TP
    key_table = w_ukey.reshape(KVLORA, HEADS, NOPE).astype(jnp.float32)
    value_table = w_uvalue.reshape(KVLORA, HEADS, VDIM).astype(jnp.float32)

    def attend(group_block):
        group_rows, latents, rotated, valid_len = group_block
        normed = rms_scale(group_rows.astype(jnp.float32), attn_gain).astype(jnp.bfloat16)
        q_small = rms_scale(jnp.dot(normed, w_qdown, preferred_element_type=jnp.float32), q_gain).astype(jnp.bfloat16)
        q_plain = jnp.dot(q_small, w_qnope, preferred_element_type=jnp.float32).astype(jnp.bfloat16).reshape(-1, HEADS, NOPE)
        q_turned = rotate(jnp.dot(q_small, w_qrope, preferred_element_type=jnp.float32).reshape(-1, HEADS, ROPE), valid_len).astype(jnp.bfloat16)
        q_latent = jnp.einsum('shn,chn->shc', q_plain.astype(jnp.float32), key_table).astype(jnp.bfloat16)
        new_latent = rms_scale(jnp.dot(normed, w_kvdown, preferred_element_type=jnp.float32), kv_gain).astype(jnp.bfloat16)
        new_rope = rotate(jnp.dot(normed, w_krope, preferred_element_type=jnp.float32), valid_len).astype(jnp.bfloat16)
        past_scores = (jnp.einsum('shc,spc->shp', q_latent.astype(jnp.float32), latents.astype(jnp.float32)) + jnp.einsum('shr,srp->shp', q_turned.astype(jnp.float32), rotated.astype(jnp.float32))) * score_scale
        in_range = jnp.arange(CACHE)[None, None, :] < valid_len[:, None, None]
        past_scores = jnp.where(in_range, past_scores, -1e+30)
        fresh_score = (lax.optimization_barrier(jnp.sum(q_latent.astype(jnp.float32) * new_latent.astype(jnp.float32)[:, None, :], axis=-1)) + lax.optimization_barrier(jnp.sum(q_turned.astype(jnp.float32) * new_rope.astype(jnp.float32)[:, None, :], axis=-1))) * score_scale
        highest = jnp.maximum(lax.optimization_barrier(jnp.max(past_scores, axis=-1)), fresh_score)
        past_exp = jnp.exp(past_scores - highest[..., None])
        fresh_exp = jnp.exp(fresh_score - highest)
        divisor = lax.optimization_barrier(jnp.sum(past_exp, axis=-1)) + fresh_exp
        past_prob = (past_exp / divisor[..., None]).astype(jnp.bfloat16)
        fresh_prob = (fresh_exp / divisor).astype(jnp.bfloat16)
        latent_mix = (jnp.einsum('shp,spc->shc', past_prob.astype(jnp.float32), latents.astype(jnp.float32)) + fresh_prob.astype(jnp.float32)[..., None] * new_latent.astype(jnp.float32)[:, None, :]).astype(jnp.bfloat16)
        head_values = jnp.einsum('shc,chv->shv', latent_mix.astype(jnp.float32), value_table).astype(jnp.bfloat16).reshape(-1, HEADS * VDIM)
        attended = jnp.zeros((head_values.shape[0], D), jnp.float32)
        for device in range(N_TP):
            block_term = jnp.dot(head_values[:, device * head_block:(device + 1) * head_block], w_out[device * head_block:(device + 1) * head_block], preferred_element_type=jnp.float32)
            attended = attended + lax.optimization_barrier(block_term.astype(jnp.bfloat16)).astype(jnp.float32)
        return attended
    attended = lax.map(attend, (hidden_in.reshape(N_EP, SEQ_GRP, D), cache_latent.reshape(N_EP, SEQ_GRP, CACHE, KVLORA), cache_rope.reshape(N_EP, SEQ_GRP, ROPE, CACHE), lengths.reshape(N_EP, SEQ_GRP))).reshape(TOKENS, D)
    residual = hidden_in.astype(jnp.float32) + attended
    normed_two = rms_scale(residual, ffn_gain).astype(jnp.bfloat16)
    group_input = normed_two.reshape(N_EP, SEQ_GRP, D)
    group_routes = routes.reshape(N_EP, SEQ_GRP, 2)
    group_slots = jax.vmap(lambda table: route_slots(table, EXPERTS))(group_routes)
    quarter_ff = FF_HALF // N_TP
    slot_range = jnp.arange(CAP, dtype=jnp.int32)

    def serve_unit(unit):
        expert = unit // 2
        chosen = (group_routes == expert)[:, None, :, :] & (group_slots[:, None, :, :] == slot_range[None, :, None, None])
        chooser = lax.optimization_barrier(jnp.sum(chosen.astype(jnp.float32), axis=-1))
        arrived = jnp.einsum('gcr,grd->gcd', chooser, group_input.astype(jnp.float32)).astype(jnp.bfloat16).reshape(N_EP * CAP, D)
        gate_part = jnp.dot(arrived, w_gate[unit], preferred_element_type=jnp.float32)
        up_part = jnp.dot(arrived, w_up[unit], preferred_element_type=jnp.float32)
        inner = (jax.nn.silu(gate_part) * up_part).astype(jnp.bfloat16)
        down_table = w_down[unit]
        summed = jnp.zeros((N_EP * CAP, D), jnp.float32)
        for device in range(N_TP):
            block_term = jnp.dot(inner[:, device * quarter_ff:(device + 1) * quarter_ff], down_table[device * quarter_ff:(device + 1) * quarter_ff], preferred_element_type=jnp.float32)
            summed = summed + lax.optimization_barrier(block_term.astype(jnp.bfloat16)).astype(jnp.float32)
        return summed.astype(jnp.bfloat16).reshape(N_EP, CAP, D)
    unit_out = lax.map(serve_unit, jnp.arange(UNITS, dtype=jnp.int32))
    group_index = jnp.arange(N_EP, dtype=jnp.int32)[:, None, None]
    first_half = unit_out[2 * group_routes, group_index, group_slots].astype(jnp.float32)
    second_half = unit_out[2 * group_routes + 1, group_index, group_slots].astype(jnp.float32)
    blended = lax.optimization_barrier(jnp.sum(route_weights.reshape(N_EP, SEQ_GRP, 2)[..., None] * (first_half + second_half), axis=2))
    return (residual + blended.reshape(TOKENS, D)).astype(jnp.bfloat16)
```

```python
import jax
import jax.numpy as jnp
from jax import lax
from jax.sharding import PartitionSpec as P

HEADS = 8
NOPE = 64
ROPE = 32
VDIM = 64
KVLORA = 128

eps = 1e-06
rope_base = 10000.0


def rms_scale(values, gain):
    return values * lax.rsqrt(jnp.mean(values * values, axis=-1, keepdims=True) + eps) * gain


def rotate(values, positions):
    width = values.shape[-1]
    middle = width // 2
    inverse = jnp.power(rope_base, -jnp.arange(0, width, 2).astype(jnp.float32) / width)
    angles = positions.astype(jnp.float32)[:, None] * inverse[None, :]
    angles = jnp.concatenate([angles, angles], axis=-1)
    target = (angles.shape[0],) + (1,) * (values.ndim - 2) + (width,)
    cosine = jnp.cos(angles).reshape(target)
    sine = jnp.sin(angles).reshape(target)
    turned = jnp.concatenate([-values[..., middle:], values[..., :middle]], axis=-1)
    return values * cosine + turned * sine


def route_slots(route_table, expert_count):
    flat_ids = route_table.reshape(-1)
    order = jnp.arange(flat_ids.shape[0])
    same = (flat_ids[:, None] == flat_ids[None, :]) & (order[None, :] < order[:, None])
    return jnp.sum(same.astype(jnp.int32), axis=1).reshape(route_table.shape)


def from_everyone(array, axis):
    copies = jnp.broadcast_to(array, (lax.axis_size(axis), *array.shape))
    return lax.all_to_all(copies, axis, split_axis=0, concat_axis=0, tiled=True)


def attention(own_rows, attn_gain, w_qdown, q_gain, w_qnope, w_qrope, w_kvdown, kv_gain, w_krope,
              w_ukey, w_uvalue, cache_latent, cache_rope, lengths):
    own_count = lengths.shape[0]
    score_scale = (NOPE + ROPE) ** (-0.5)
    normed = rms_scale(own_rows, attn_gain).astype(jnp.bfloat16)
    q_small = rms_scale(
        jnp.dot(normed, w_qdown, preferred_element_type=jnp.float32), q_gain
    ).astype(jnp.bfloat16)
    q_plain = (
        jnp.dot(q_small, w_qnope, preferred_element_type=jnp.float32)
        .astype(jnp.bfloat16)
        .reshape(own_count, HEADS, NOPE)
    )
    q_turned = rotate(
        jnp.dot(q_small, w_qrope, preferred_element_type=jnp.float32).reshape(
            own_count, HEADS, ROPE
        ),
        lengths,
    ).astype(jnp.bfloat16)
    q_latent = jnp.einsum(
        "shn,chn->shc",
        q_plain,
        w_ukey.reshape(KVLORA, HEADS, NOPE),
        preferred_element_type=jnp.float32,
    ).astype(jnp.bfloat16)
    new_latent = rms_scale(
        jnp.dot(normed, w_kvdown, preferred_element_type=jnp.float32), kv_gain
    ).astype(jnp.bfloat16)
    new_rope = rotate(jnp.dot(normed, w_krope, preferred_element_type=jnp.float32), lengths).astype(
        jnp.bfloat16
    )
    past_scores = (
        jnp.einsum("shc,spc->shp", q_latent, cache_latent, preferred_element_type=jnp.float32)
        + jnp.einsum("shr,srp->shp", q_turned, cache_rope, preferred_element_type=jnp.float32)
    ) * score_scale
    in_range = jnp.arange(cache_latent.shape[1])[None, None, :] < lengths[:, None, None]
    past_scores = jnp.where(in_range, past_scores, -1e30)
    fresh_score = (
        jnp.einsum("shc,sc->sh", q_latent, new_latent, preferred_element_type=jnp.float32)
        + jnp.einsum("shr,sr->sh", q_turned, new_rope, preferred_element_type=jnp.float32)
    ) * score_scale
    highest = jnp.maximum(jnp.max(past_scores, axis=-1), fresh_score)
    past_exp = jnp.exp(past_scores - highest[..., None])
    fresh_exp = jnp.exp(fresh_score - highest)
    divisor = jnp.sum(past_exp, axis=-1) + fresh_exp
    past_prob = (past_exp / divisor[..., None]).astype(jnp.bfloat16)
    fresh_prob = (fresh_exp / divisor).astype(jnp.bfloat16)
    latent_mix = (
        jnp.einsum("shp,spc->shc", past_prob, cache_latent, preferred_element_type=jnp.float32)
        + fresh_prob.astype(jnp.float32)[..., None] * new_latent.astype(jnp.float32)[:, None, :]
    ).astype(jnp.bfloat16)
    return (
        jnp.einsum(
            "shc,chv->shv",
            latent_mix,
            w_uvalue.reshape(KVLORA, HEADS, VDIM),
            preferred_element_type=jnp.float32,
        )
        .astype(jnp.bfloat16)
        .reshape(own_count, HEADS * VDIM)
    )


def per_device(
    hidden_in, attn_gain, w_qdown, q_gain, w_qnope, w_qrope, w_kvdown, kv_gain, w_krope, w_ukey,
    w_uvalue, w_out, cache_latent, cache_rope, lengths, ffn_gain, routes, route_weights, w_gate,
    w_up, w_down,
):
    group_rows, width = hidden_in.shape
    own_count = lengths.shape[0]
    tp = lax.axis_size("tp")
    ep = lax.axis_size("ep")
    experts = ep // 2
    capacity = 2
    quarter = width // tp
    block = quarter // 2
    tp_rank = lax.axis_index("tp")
    core = lax.axis_index("ep") % 2
    columns = [[(2 * k + c) * tp + t for c in range(2) for t in range(tp)] for k in range(experts)]
    same_core = [[2 * k + c for k in range(experts)] for c in range(2)]
    pairs = [[2 * k, 2 * k + 1] for k in range(experts)]

    w_all = from_everyone(w_out, "tp")
    own_rows = lax.dynamic_slice_in_dim(hidden_in, tp_rank * own_count, own_count, 0).astype(
        jnp.float32
    )
    head_values = attention(
        own_rows, attn_gain, w_qdown, q_gain, w_qnope, w_qrope, w_kvdown, kv_gain, w_krope,
        w_ukey, w_uvalue, cache_latent, cache_rope, lengths,
    )
    terms = jnp.einsum(
        "sbf,bfd->bsd",
        head_values.reshape(own_count, tp, -1),
        w_all,
        preferred_element_type=jnp.float32,
    ).astype(jnp.bfloat16)
    attended = jnp.sum(terms.astype(jnp.float32), axis=0)
    residual = own_rows + attended
    normed_two = rms_scale(residual, ffn_gain).astype(jnp.bfloat16)

    slots = route_slots(routes, experts)
    targets = routes * (2 * capacity) + core * capacity + slots
    meta = jnp.concatenate([targets.astype(jnp.float32), route_weights], axis=1)
    meta = lax.dynamic_slice_in_dim(meta, tp_rank * own_count, own_count, 0)
    meta = jnp.pad(meta, ((0, 0), (0, 124)))
    normed_blocks = normed_two.astype(jnp.float32).reshape(own_count, tp, 2, block)
    outgoing = jnp.concatenate(
        [
            jnp.broadcast_to(
                residual.reshape(own_count, tp, quarter).transpose(1, 0, 2)[None],
                (2, tp, own_count, quarter),
            ),
            normed_blocks.transpose(2, 1, 0, 3),
            jnp.broadcast_to(meta[None, None], (2, tp, own_count, 128)),
        ],
        axis=-1,
    ).reshape(2 * tp, own_count, quarter + block + 128)
    inbox = lax.all_to_all(
        outgoing, ("ep", "tp"), 0, 0, axis_index_groups=columns, tiled=True
    ).reshape(2 * group_rows, quarter + block + 128)
    own_columns = lax.dynamic_slice_in_dim(inbox, core * group_rows, group_rows, 0)[:, :quarter]
    chip_rows = inbox[:, quarter : quarter + block].astype(jnp.bfloat16)
    chip_targets = inbox[:, quarter + block : quarter + block + 2].astype(jnp.int32)
    chip_weights = inbox[:, quarter + block + 2 : quarter + block + 4]

    rows = experts * 2 * capacity
    picks = chip_targets[:, :, None] == jnp.arange(rows)[None, None, :]
    chooser = jnp.sum(picks.astype(jnp.float32), axis=1).astype(jnp.bfloat16)
    sent = jnp.einsum("ru,rd->ud", chooser, chip_rows, preferred_element_type=jnp.float32).astype(
        jnp.bfloat16
    )
    arrived = lax.all_to_all(
        sent.reshape(experts, 2 * capacity, block), "ep", 0, 0, axis_index_groups=same_core,
        tiled=True,
    ).reshape(rows, block)
    over_tp = from_everyone(arrived, "tp")
    both = lax.all_gather(over_tp, "ep", axis_index_groups=pairs)
    joined = both.transpose(2, 1, 0, 3).reshape(rows, width)
    gate_part = jnp.dot(joined, w_gate[0], preferred_element_type=jnp.float32)
    up_part = jnp.dot(joined, w_up[0], preferred_element_type=jnp.float32)
    inner = (jax.nn.silu(gate_part) * up_part).astype(jnp.bfloat16)
    block_term = jnp.dot(inner, w_down[0], preferred_element_type=jnp.float32).astype(jnp.bfloat16)
    pieces = lax.all_to_all(
        block_term.reshape(rows, tp, quarter).transpose(1, 0, 2), "tp", 0, 0, tiled=True
    )
    half_out = jnp.sum(pieces.astype(jnp.float32), axis=0).astype(jnp.bfloat16)
    returned = lax.all_to_all(
        half_out.reshape(experts, 2 * capacity, quarter), "ep", 0, 0, axis_index_groups=same_core,
        tiled=True,
    ).reshape(rows, quarter)
    chosen = jnp.einsum(
        "rku,ud->rkd", picks.astype(jnp.bfloat16), returned, preferred_element_type=jnp.float32
    )
    blended = jnp.sum(chip_weights[:, :, None] * chosen, axis=1)
    others = lax.dynamic_slice_in_dim(blended, (1 - core) * group_rows, group_rows, 0)
    mine = lax.dynamic_slice_in_dim(blended, core * group_rows, group_rows, 0)
    swapped = lax.all_gather(others, "ep", axis_index_groups=pairs)
    partner = lax.dynamic_index_in_dim(swapped, 1 - core, 0, keepdims=False)
    return (own_columns + (mine + partner)).astype(jnp.bfloat16)


def solution(mesh):
    placed = (
        P("ep", None),
        P(),
        P(),
        P(),
        P(),
        P(),
        P(),
        P(),
        P(),
        P(),
        P(),
        P("tp", None),
        P(("ep", "tp"), None, None),
        P(("ep", "tp"), None, None),
        P(("ep", "tp")),
        P(),
        P("ep", None),
        P("ep", None),
        P("ep", None, "tp"),
        P("ep", None, "tp"),
        P("ep", "tp", None),
    )
    return jax.shard_map(
        per_device, mesh=mesh, in_specs=placed, out_specs=P("ep", "tp"), check_vma=False
    )
```

```python
import jax
import jax.numpy as jnp
from jax import lax
from jax.experimental import pallas as pl
from jax.experimental.pallas import tpu as pltpu
from jax.sharding import PartitionSpec as P

HEADS = 8
NOPE = 64
ROPE = 32
VDIM = 64
KVLORA = 128

eps = 1e-06
rope_base = 10000.0
VMEM = pl.BlockSpec(memory_space=pltpu.VMEM)
SMEM = pl.BlockSpec(memory_space=pltpu.SMEM)
NT = (((1,), (1,)), ((), ()))
TN = (((0,), (0,)), ((), ()))
f32 = jnp.float32
bf16 = jnp.bfloat16


def dot(a, b, dims=(((1,), (0,)), ((), ()))):
    return lax.dot_general(a, b, dims, preferred_element_type=f32)


def iota(shape, dim):
    return lax.broadcasted_iota(jnp.int32, shape, dim)


def rms(values, gain):
    return values * lax.rsqrt(jnp.mean(values * values, axis=-1, keepdims=True) + eps) * gain


def turn(values, cosine, sine):
    width = values.shape[-1]
    lanes = iota(values.shape, 1) % ROPE
    ahead = pltpu.roll(values, width - ROPE // 2, 1)
    behind = pltpu.roll(values, ROPE // 2, 1)
    turned = jnp.where(lanes < ROPE // 2, -ahead, behind)
    return values * cosine + turned * sine


def attend_kernel(
    lengths, hidden, attn_gain, q_gain, kv_gain, table, routes, wqd, wqn, wqr, wkv, wkr, wuk, wuv,
    latent, rope, payload, mixed,
):
    own = latent.shape[0]
    rows = hidden.shape[0]
    tp = rows // own
    quarter = hidden.shape[1] // tp
    t = lax.axis_index("tp")
    c = lax.axis_index("ep") % 2
    r0, r1 = routes[0:1, :], routes[1:2, :]
    row, col = iota((rows, rows), 0), iota((rows, rows), 1)
    earlier = col < row
    ids = []
    for line in (r0, r1):
        mine = jnp.sum(jnp.where(row == col, line, 0), axis=1, keepdims=True)
        hits = (jnp.where(r0 == mine, 1, 0) + jnp.where(r1 == mine, 1, 0)) * jnp.where(
            earlier, 1, 0
        )
        slot = jnp.sum(hits, axis=1, keepdims=True)
        ids.append(mine * 4 + c * 2 + slot)
    lane = iota((rows, 128), 1)
    meta = jnp.where(lane == 0, ids[0], jnp.where(lane == 1, ids[1], 0)).astype(f32).astype(bf16)
    pick = jnp.where(
        (iota((8, rows), 1) == t * own + iota((8, rows), 0)) & (iota((8, rows), 0) < own), 1.0, 0.0
    ).astype(bf16)
    own_hidden = dot(pick, hidden[...])
    own_meta = dot(pick, meta)
    normed = rms(own_hidden, attn_gain[...]).astype(bf16)
    q_small = rms(dot(normed, wqd[...]), q_gain[...]).astype(bf16)
    q_plain = dot(q_small, wqn[...])
    cosine, sine = table[0], table[1]
    q_turned = turn(dot(q_small, wqr[...]), cosine, sine)
    new_latent = rms(dot(normed, wkv[...]), kv_gain[...]).astype(bf16).astype(f32)
    plain_key = dot(normed, wkr[...], NT)
    swap = jnp.concatenate([-plain_key[:, ROPE // 2 :], plain_key[:, : ROPE // 2]], axis=1)
    new_rope = (
        (plain_key * cosine[:, :ROPE] + swap * sine[:, :ROPE]).astype(bf16).astype(f32)
    )

    def spread(values, size):
        width = values.shape[1]
        head = iota((HEADS, width), 1) // size
        mask = head == iota((HEADS, width), 0)
        return jnp.concatenate(
            [jnp.where(mask, values[s : s + 1, :], 0.0) for s in range(own)], axis=0
        ).astype(bf16)

    q_latent = dot(spread(q_plain, NOPE), wuk[...], NT).astype(bf16)
    fold = jnp.where(
        iota((HEADS * ROPE, ROPE), 0) % ROPE == iota((HEADS * ROPE, ROPE), 1), 1.0, 0.0
    ).astype(bf16)
    q_rope = dot(spread(q_turned, ROPE), fold).astype(bf16)
    scale = (NOPE + ROPE) ** (-0.5)
    for s in range(own):
        mine = slice(s * HEADS, (s + 1) * HEADS)
        scores = (
            dot(q_latent[mine], latent[s], NT) + dot(q_rope[mine], rope[s])
        ) * scale
        scores = jnp.where(iota(scores.shape, 1) < lengths[s], scores, -1e30)
        fresh = (
            jnp.sum(q_latent[mine].astype(f32) * new_latent[s : s + 1, :], axis=1, keepdims=True)
            + jnp.sum(q_rope[mine].astype(f32) * new_rope[s : s + 1, :], axis=1, keepdims=True)
        ) * scale
        highest = jnp.maximum(jnp.max(scores, axis=1, keepdims=True), fresh)
        past = jnp.exp(scores - highest)
        now = jnp.exp(fresh - highest)
        divisor = jnp.sum(past, axis=1, keepdims=True) + now
        mix = dot((past / divisor).astype(bf16), latent[s])
        mix = mix + (now / divisor).astype(bf16).astype(f32) * new_latent[s : s + 1, :]
        mixed[mine, :] = mix.astype(bf16).astype(f32)
    values = dot(mixed[...].astype(bf16), wuv[...])
    head = iota((HEADS, HEADS * VDIM), 1) // VDIM == iota((HEADS, HEADS * VDIM), 0)
    head_values = jnp.concatenate(
        [
            jnp.sum(
                jnp.where(head, values[s * HEADS : (s + 1) * HEADS], 0.0), axis=0, keepdims=True
            )
            for s in range(own)
        ],
        axis=0,
    ).astype(bf16)
    width = HEADS * VDIM
    own_hidden = own_hidden[:own].astype(bf16)
    own_meta = own_meta[:own].astype(bf16)
    for j in range(2 * tp):
        payload[j, :, :width] = head_values
        payload[j, :, width : width + quarter] = own_hidden[
            :, (j % tp) * quarter : (j % tp + 1) * quarter
        ]
        payload[j, :, width + quarter :] = own_meta


def project_kernel(inbox, w, sent, residual_out, ids_out):
    c = lax.axis_index("ep") % 2
    rows = inbox.shape[0]
    tp, depth, quarter = w.shape
    width = tp * depth
    total = jnp.zeros((rows, quarter), f32)
    for b in range(tp):
        total = total + dot(inbox[:, b * depth : (b + 1) * depth], w[b]).astype(bf16).astype(f32)
    residual = inbox[:, width : width + quarter].astype(f32) + total
    half = quarter // 2
    block = jnp.where(c == 0, residual[:, :half], residual[:, half:]).astype(bf16)
    meta = inbox[:, width + quarter :].astype(f32).astype(jnp.int32)
    lanes = iota((rows, sent.shape[0]), 1)
    chooser = jnp.where((meta[:, 0:1] == lanes) | (meta[:, 1:2] == lanes), 1.0, 0.0).astype(bf16)
    sent[...] = dot(chooser, block, TN).astype(bf16)
    group = rows // 2
    residual_out[...] = jnp.where(c == 0, residual[:group], residual[group:])
    ids_out[...] = meta


def expert_kernel(both, gain, wg, wu, wd, out, x):
    cores, tp, rows, block = both.shape
    quarter = cores * block
    for part in range(2):
        size = rows // 2
        here = slice(part * size, (part + 1) * size)
        values = jnp.concatenate(
            [both[n, t, here, :] for t in range(tp) for n in range(cores)], axis=1
        ).astype(f32)
        x[here, :] = rms(values, gain[...]).astype(bf16)
    gate = dot(x[...], wg[...], NT)
    up = dot(x[...], wu[...], NT)
    inner = (gate / (1.0 + jnp.exp(-gate)) * up).astype(bf16)
    for t in range(tp):
        out[t] = dot(inner, wd[:, t * quarter : (t + 1) * quarter]).astype(bf16)


def combine_kernel(returned, ids, send, keep):
    c = lax.axis_index("ep") % 2
    rows = ids.shape[0]
    group = rows // 2
    lanes = iota((rows, returned.shape[0]), 1)
    for k in range(2):
        chooser = jnp.where(ids[:, k : k + 1] == lanes, 1.0, 0.0).astype(bf16)
        chosen = dot(chooser, returned[...])
        first, second = chosen[:group], chosen[group:]
        send[k] = jnp.where(c == 0, second, first).astype(bf16)
        keep[k] = jnp.where(c == 0, first, second)


def finish_kernel(swapped, keep, residual, weights, out):
    c = lax.axis_index("ep") % 2
    rows = residual.shape[0]
    same = iota((rows, rows), 0) == iota((rows, rows), 1)
    blended = jnp.zeros(residual.shape, f32)
    for k in range(2):
        partner = jnp.where(c == 0, swapped[1, k].astype(f32), swapped[0, k].astype(f32))
        weight = jnp.sum(jnp.where(same, weights[k : k + 1, :], 0.0), axis=1, keepdims=True)
        blended = blended + weight * (keep[k] + partner)
    out[...] = (residual[...] + blended).astype(bf16)


def per_device(
    hidden_in, attn_gain, w_qdown, q_gain, w_qnope, w_qrope, w_kvdown, kv_gain, w_krope, w_ukey,
    w_uvalue, w_out, cache_latent, cache_rope, lengths, ffn_gain, routes, route_weights, w_gate,
    w_up, w_down,
):
    group_rows, width = hidden_in.shape
    own = lengths.shape[0]
    tp = lax.axis_size("tp")
    experts = lax.axis_size("ep") // 2
    quarter = width // tp
    block = quarter // 2
    columns = [[(2 * k + c) * tp + t for c in range(2) for t in range(tp)] for k in range(experts)]
    same_core = [[2 * k + c for k in range(experts)] for c in range(2)]
    pairs = [[2 * k, 2 * k + 1] for k in range(experts)]

    w_mine = lax.all_to_all(
        jnp.stack([w_out[:, n * quarter : (n + 1) * quarter] for n in range(tp)]),
        "tp", 0, 0, tiled=True,
    )
    inverse = jnp.power(rope_base, -jnp.arange(0, ROPE, 2).astype(f32) / ROPE)
    positions = jnp.pad(lengths, (0, 8 - own)).astype(f32)
    angles = positions[:, None] * jnp.tile(inverse, 2 * HEADS)[None, :]
    table = jnp.stack([jnp.cos(angles), jnp.sin(angles)])
    wide = HEADS * VDIM + quarter + 128
    big = [hidden_in, w_qdown, w_qnope, w_qrope, w_kvdown, w_krope.T, w_ukey, w_uvalue,
           cache_latent, cache_rope]
    attend = pl.pallas_call(
        attend_kernel,
        out_shape=jax.ShapeDtypeStruct((2 * tp, own, wide), bf16),
        in_specs=[SMEM] + [VMEM] * 15,
        out_specs=VMEM,
        scratch_shapes=[pltpu.VMEM((own * HEADS, KVLORA), f32)],
        cost_estimate=pl.CostEstimate(
            flops=20_000_000_000, bytes_accessed=3_000_000, transcendentals=40_000
        ),
        compiler_params=pltpu.CompilerParams(vmem_limit_bytes=12 << 20),
        name="attend",
    )
    payload = attend(
        lengths, hidden_in, attn_gain[None], q_gain[None], kv_gain[None], table, routes.T,
        *big[1:],
    )
    payload, w_mine = lax.optimization_barrier((payload, w_mine))
    inbox = lax.all_to_all(
        payload, ("ep", "tp"), 0, 0, axis_index_groups=columns, tiled=True
    ).reshape(2 * group_rows, wide)
    rows = experts * 4
    sent, residual, ids = pl.pallas_call(
        project_kernel,
        out_shape=[
            jax.ShapeDtypeStruct((rows, block), bf16),
            jax.ShapeDtypeStruct((group_rows, quarter), f32),
            jax.ShapeDtypeStruct((2 * group_rows, 128), jnp.int32),
        ],
        in_specs=[VMEM] * 2,
        out_specs=[VMEM] * 3,
        compiler_params=pltpu.CompilerParams(vmem_limit_bytes=8 << 20),
        name="project",
    )(inbox, w_mine)
    arrived = lax.all_to_all(
        sent.reshape(experts, 4, block), "ep", 0, 0, axis_index_groups=same_core, tiled=True
    ).reshape(rows, block)
    over_tp = lax.all_to_all(
        jnp.broadcast_to(arrived, (tp, rows, block)), "tp", 0, 0, tiled=True
    )
    both = lax.all_gather(over_tp, "ep", axis_index_groups=pairs)
    partial = pl.pallas_call(
        expert_kernel,
        out_shape=jax.ShapeDtypeStruct((tp, rows, quarter), bf16),
        in_specs=[VMEM] * 5,
        out_specs=VMEM,
        scratch_shapes=[pltpu.VMEM((rows, width), bf16)],
        compiler_params=pltpu.CompilerParams(vmem_limit_bytes=20 << 20),
        name="expert",
    )(both, ffn_gain[None], jnp.swapaxes(w_gate[0], 0, 1), jnp.swapaxes(w_up[0], 0, 1), w_down[0])
    pieces = lax.all_to_all(partial, "tp", 0, 0, tiled=True)
    half_out = jnp.sum(pieces.astype(f32), axis=0).astype(bf16)
    returned = lax.all_to_all(
        half_out.reshape(experts, 4, quarter), "ep", 0, 0, axis_index_groups=same_core, tiled=True
    ).reshape(rows, quarter)
    send, keep = pl.pallas_call(
        combine_kernel,
        out_shape=[
            jax.ShapeDtypeStruct((2, group_rows, quarter), bf16),
            jax.ShapeDtypeStruct((2, group_rows, quarter), f32),
        ],
        in_specs=[VMEM] * 2,
        out_specs=[VMEM] * 2,
        compiler_params=pltpu.CompilerParams(vmem_limit_bytes=8 << 20),
        name="combine",
    )(returned, ids)
    swapped = lax.all_gather(send, "ep", axis_index_groups=pairs)
    return pl.pallas_call(
        finish_kernel,
        out_shape=jax.ShapeDtypeStruct((group_rows, quarter), bf16),
        in_specs=[VMEM] * 4,
        out_specs=VMEM,
        compiler_params=pltpu.CompilerParams(vmem_limit_bytes=8 << 20),
        name="finish",
    )(swapped, keep, residual, route_weights.T)


def solution(mesh):
    placed = (
        P("ep", None),
        P(),
        P(),
        P(),
        P(),
        P(),
        P(),
        P(),
        P(),
        P(),
        P(),
        P("tp", None),
        P(("ep", "tp"), None, None),
        P(("ep", "tp"), None, None),
        P(("ep", "tp")),
        P(),
        P("ep", None),
        P("ep", None),
        P("ep", None, "tp"),
        P("ep", None, "tp"),
        P("ep", "tp", None),
    )
    return jax.shard_map(
        per_device, mesh=mesh, in_specs=placed, out_specs=P("ep", "tp"), check_vma=False
    )
```

```python
import jax
import jax.numpy as jnp
from jax import lax
from jax.experimental import pallas as pl
from jax.experimental.pallas import tpu as pltpu
from jax.sharding import PartitionSpec as P

HEADS = 8
NOPE = 64
ROPE = 32
VDIM = 64
KVLORA = 128

eps = 1e-06
rope_base = 10000.0
VMEM = pl.BlockSpec(memory_space=pltpu.VMEM)
HBM = pl.BlockSpec(memory_space=pltpu.HBM)
SMEM = pl.BlockSpec(memory_space=pltpu.SMEM)
NT = (((1,), (1,)), ((), ()))
TN = (((0,), (0,)), ((), ()))
f32 = jnp.float32
bf16 = jnp.bfloat16


def dot(a, b, dims=(((1,), (0,)), ((), ()))):
    return lax.dot_general(a, b, dims, preferred_element_type=f32)


def iota(shape, dim):
    return lax.broadcasted_iota(jnp.int32, shape, dim)


def rms(values, gain):
    return values * lax.rsqrt(jnp.mean(values * values, axis=-1, keepdims=True) + eps) * gain


def turn(values, cosine, sine):
    width = values.shape[-1]
    lanes = iota(values.shape, 1) % ROPE
    ahead = pltpu.roll(values, width - ROPE // 2, 1)
    behind = pltpu.roll(values, ROPE // 2, 1)
    turned = jnp.where(lanes < ROPE // 2, -ahead, behind)
    return values * cosine + turned * sine


def attend_kernel(
    lengths, attn_gain, q_gain, kv_gain, ffn_gain, table, routes, weights, h_hidden, h_wqd, h_wqn,
    h_wqr, h_wkv, h_wkr, h_wuk, h_rope, h_latent, h_wuv, h_wout, payload, gain_out, hidden, wqd,
    wqn, wqr, wkv, wkr, wuk, rope, latent, wuv, mixed, sems,
):
    own = latent.shape[0]
    rows, width = hidden.shape
    tp = rows // own
    block = width // (2 * tp)
    part = h_wout.shape[0] // 2
    t = lax.axis_index("tp")
    c = lax.axis_index("ep") % 2
    pairs = [
        (h_hidden, hidden), (h_wqd, wqd), (h_wqn, wqn), (h_wqr, wqr), (h_wkv, wkv), (h_wkr, wkr),
        (h_wuk, wuk), (h_rope, rope), (h_latent, latent), (h_wuv, wuv),
    ]
    copies = [pltpu.make_async_copy(src, dst, sems.at[n]) for n, (src, dst) in enumerate(pairs)]
    for j in range(2 * tp):
        column = (2 * (j % tp) + j // tp) * block
        copies.append(
            pltpu.make_async_copy(
                h_wout.at[pl.ds(pl.multiple_of(c * part, part), part), column : column + block],
                payload.at[j, 0:part, :],
                sems.at[len(copies)],
            )
        )
    for copy in copies:
        copy.start()
    gain_out[...] = ffn_gain[...]
    r0, r1 = routes[0:1, :], routes[1:2, :]
    row, col = iota((rows, rows), 0), iota((rows, rows), 1)
    earlier = col < row
    ids = []
    for line in (r0, r1):
        mine = jnp.sum(jnp.where(row == col, line, 0), axis=1, keepdims=True)
        hits = (jnp.where(r0 == mine, 1, 0) + jnp.where(r1 == mine, 1, 0)) * jnp.where(
            earlier, 1, 0
        )
        slot = jnp.sum(hits, axis=1, keepdims=True)
        ids.append(mine * 4 + c * 2 + slot)
    lane = iota((rows, 128), 1)
    meta = jnp.where(lane == 0, ids[0], jnp.where(lane == 1, ids[1], 0)).astype(f32)
    for k in range(2):
        rest = jnp.sum(jnp.where(row == col, weights[k : k + 1, :], 0.0), axis=1, keepdims=True)
        for n in range(3):
            piece = rest.astype(bf16).astype(f32)
            meta = jnp.where(lane == 2 + 3 * k + n, piece, meta)
            rest = rest - piece
    meta = meta.astype(bf16)
    pick = jnp.where(
        (iota((8, rows), 1) == t * own + iota((8, rows), 0)) & (iota((8, rows), 0) < own), 1.0, 0.0
    ).astype(bf16)
    copies[0].wait()
    own_hidden = dot(pick, hidden[...])
    own_meta = dot(pick, meta)
    normed = rms(own_hidden, attn_gain[...]).astype(bf16)
    copies[1].wait()
    q_small = rms(dot(normed, wqd[...]), q_gain[...]).astype(bf16)
    copies[2].wait()
    q_plain = dot(q_small, wqn[...])
    cosine, sine = table[0], table[1]
    copies[3].wait()
    q_turned = turn(dot(q_small, wqr[...]), cosine, sine)
    copies[4].wait()
    new_latent = rms(dot(normed, wkv[...]), kv_gain[...]).astype(bf16).astype(f32)
    copies[5].wait()
    plain_key = dot(normed, wkr[...], NT)
    swap = jnp.concatenate([-plain_key[:, ROPE // 2 :], plain_key[:, : ROPE // 2]], axis=1)
    new_rope = (
        (plain_key * cosine[:, :ROPE] + swap * sine[:, :ROPE]).astype(bf16).astype(f32)
    )

    def spread(values, size):
        width = values.shape[1]
        head = iota((HEADS, width), 1) // size
        mask = head == iota((HEADS, width), 0)
        return jnp.concatenate(
            [jnp.where(mask, values[s : s + 1, :], 0.0) for s in range(own)], axis=0
        ).astype(bf16)

    copies[6].wait()
    q_latent = dot(spread(q_plain, NOPE), wuk[...], NT).astype(bf16)
    fold = jnp.where(
        iota((HEADS * ROPE, ROPE), 0) % ROPE == iota((HEADS * ROPE, ROPE), 1), 1.0, 0.0
    ).astype(bf16)
    q_rope = dot(spread(q_turned, ROPE), fold).astype(bf16)
    scale = (NOPE + ROPE) ** (-0.5)
    copies[7].wait()
    copies[8].wait()
    for s in range(own):
        mine = slice(s * HEADS, (s + 1) * HEADS)
        scores = (
            dot(q_latent[mine], latent[s], NT) + dot(q_rope[mine], rope[s])
        ) * scale
        scores = jnp.where(iota(scores.shape, 1) < lengths[s], scores, -1e30)
        fresh = (
            jnp.sum(q_latent[mine].astype(f32) * new_latent[s : s + 1, :], axis=1, keepdims=True)
            + jnp.sum(q_rope[mine].astype(f32) * new_rope[s : s + 1, :], axis=1, keepdims=True)
        ) * scale
        highest = jnp.maximum(jnp.max(scores, axis=1, keepdims=True), fresh)
        past = jnp.exp(scores - highest)
        now = jnp.exp(fresh - highest)
        divisor = jnp.sum(past, axis=1, keepdims=True) + now
        mix = dot((past / divisor).astype(bf16), latent[s])
        mix = mix + (now / divisor).astype(bf16).astype(f32) * new_latent[s : s + 1, :]
        mixed[mine, :] = mix.astype(bf16).astype(f32)
    copies[9].wait()
    values = dot(mixed[...].astype(bf16), wuv[...])
    head = iota((HEADS, HEADS * VDIM), 1) // VDIM == iota((HEADS, HEADS * VDIM), 0)
    head_values = jnp.concatenate(
        [
            jnp.sum(
                jnp.where(head, values[s * HEADS : (s + 1) * HEADS], 0.0), axis=0, keepdims=True
            )
            for s in range(own)
        ],
        axis=0,
    )
    parts = [
        head_values[:, b * (HEADS * VDIM // tp) : (b + 1) * (HEADS * VDIM // tp)]
        for b in range(tp)
    ]
    for j in range(2 * tp):
        column = (2 * (j % tp) + j // tp) * block
        payload[j, part:, :] = jnp.concatenate(
            [*parts, own_hidden[:own, column : column + block], own_meta[:own]], axis=0
        ).astype(bf16)
    for copy in copies[len(pairs) :]:
        copy.wait()


def project_kernel(inbox, sent, residual_out, meta_out):
    devices, lines, block = inbox.shape
    tp = devices // 2
    own = 4
    part = lines - own * (tp + 2)
    tails = [inbox[j, part:, :].astype(f32) for j in range(devices)]

    def section(n):
        return jnp.concatenate([tail[n * own : (n + 1) * own] for tail in tails], axis=0)

    total = jnp.zeros((devices * own, block), f32)
    for b in range(tp):
        w = jnp.concatenate([inbox[b, :part, :], inbox[tp + b, :part, :]], axis=0)
        total = total + dot(section(b).astype(bf16), w).astype(bf16).astype(f32)
    residual = section(tp) + total
    meta = section(tp + 1)
    targets = meta.astype(jnp.int32)
    lanes = iota((devices * own, sent.shape[0]), 1)
    chooser = jnp.where(
        (targets[:, 0:1] == lanes) | (targets[:, 1:2] == lanes), 1.0, 0.0
    ).astype(bf16)
    sent[...] = dot(chooser, residual.astype(bf16), TN).astype(bf16)
    residual_out[...] = residual
    meta_out[...] = meta


def expert_kernel(both, gain, wg, wu, wd, stay, away, x):
    c = lax.axis_index("ep") % 2
    cores, tp, rows, block = both.shape
    quarter = cores * block
    for part in range(2):
        size = rows // 2
        here = slice(part * size, (part + 1) * size)
        values = jnp.concatenate(
            [both[n, t, here, :] for t in range(tp) for n in range(cores)], axis=1
        ).astype(f32)
        x[here, :] = rms(values, gain[...]).astype(bf16)
    gate = dot(x[...], wg[...], NT)
    up = dot(x[...], wu[...], NT)
    inner = (gate / (1.0 + jnp.exp(-gate)) * up).astype(bf16)
    for t in range(tp):
        term = dot(inner, wd[:, t * quarter : (t + 1) * quarter])
        first, second = term[:, :block], term[:, block:]
        stay[t] = jnp.where(c == 0, first, second).astype(bf16)
        away[t] = jnp.where(c == 0, second, first).astype(bf16)


def pair_kernel(stay, swapped, out):
    partner = 1 - lax.axis_index("ep") % 2
    for t in range(stay.shape[0]):
        out[t] = (stay[t].astype(f32) + swapped[partner, t].astype(f32)).astype(bf16)


def combine_kernel(returned, meta, residual, send, keep):
    c = lax.axis_index("ep") % 2
    rows = meta.shape[0]
    group = rows // 2
    targets = meta[...].astype(jnp.int32)
    lanes = iota((rows, returned.shape[0]), 1)
    blended = jnp.zeros(residual.shape, f32)
    for k in range(2):
        chooser = jnp.where(targets[:, k : k + 1] == lanes, 1.0, 0.0).astype(bf16)
        first = 2 + 3 * k
        weight = (meta[:, first : first + 1] + meta[:, first + 1 : first + 2]) + meta[
            :, first + 2 : first + 3
        ]
        blended = blended + weight * dot(chooser, returned[...])
    total = residual[...] + blended
    send[...] = jnp.where(c == 0, total[group:], total[:group]).astype(bf16)
    keep[...] = jnp.where(c == 0, total[:group], total[group:])


def finish_kernel(swapped, keep, out):
    c = lax.axis_index("ep") % 2
    block = keep.shape[1]
    mine = keep[...]
    out[:, :block] = jnp.where(c == 0, mine, swapped[0].astype(f32)).astype(bf16)
    out[:, block:] = jnp.where(c == 0, swapped[1].astype(f32), mine).astype(bf16)


def per_device(
    hidden_in, attn_gain, w_qdown, q_gain, w_qnope, w_qrope, w_kvdown, kv_gain, w_krope, w_ukey,
    w_uvalue, w_out, cache_latent, cache_rope, lengths, ffn_gain, routes, route_weights, w_gate,
    w_up, w_down,
):
    group_rows, width = hidden_in.shape
    own = lengths.shape[0]
    tp = lax.axis_size("tp")
    experts = lax.axis_size("ep") // 2
    quarter = width // tp
    block = quarter // 2
    columns = [[(2 * k + c) * tp + t for c in range(2) for t in range(tp)] for k in range(experts)]
    same_core = [[2 * k + c for k in range(experts)] for c in range(2)]
    pairs = [[2 * k, 2 * k + 1] for k in range(experts)]

    inverse = jnp.power(rope_base, -jnp.arange(0, ROPE, 2).astype(f32) / ROPE)
    positions = jnp.pad(lengths, (0, 8 - own)).astype(f32)
    angles = positions[:, None] * jnp.tile(inverse, 2 * HEADS)[None, :]
    table = jnp.stack([jnp.cos(angles), jnp.sin(angles)])
    big = [hidden_in, w_qdown, w_qnope, w_qrope, w_kvdown, w_krope.T, w_ukey, cache_rope,
           cache_latent, w_uvalue]
    lines = w_out.shape[0] // 2 + own * (tp + 2)
    rows = experts * 4
    small_vmem = pltpu.CompilerParams(vmem_limit_bytes=8 << 20)
    payload, gain = pl.pallas_call(
        attend_kernel,
        out_shape=[
            jax.ShapeDtypeStruct((2 * tp, lines, block), bf16),
            jax.ShapeDtypeStruct((1, width), f32),
        ],
        in_specs=[SMEM] + [VMEM] * 7 + [HBM] * 11,
        out_specs=[VMEM] * 2,
        scratch_shapes=[pltpu.VMEM(a.shape, a.dtype) for a in big]
        + [pltpu.VMEM((own * HEADS, KVLORA), f32)]
        + [pltpu.SemaphoreType.DMA((len(big) + 2 * tp,))],
        compiler_params=pltpu.CompilerParams(vmem_limit_bytes=12 << 20),
        name="attend",
    )(
        lengths, attn_gain[None], q_gain[None], kv_gain[None], ffn_gain[None], table, routes.T,
        route_weights.T, *[pltpu.with_memory_space_constraint(a, pltpu.HBM) for a in [*big, w_out]],
    )
    inbox = lax.all_to_all(
        payload, ("ep", "tp"), 0, 0, axis_index_groups=columns, tiled=True
    )
    sent, residual, meta = pl.pallas_call(
        project_kernel,
        out_shape=[
            jax.ShapeDtypeStruct((rows, block), bf16),
            jax.ShapeDtypeStruct((2 * group_rows, block), f32),
            jax.ShapeDtypeStruct((2 * group_rows, 128), f32),
        ],
        in_specs=[VMEM],
        out_specs=[VMEM] * 3,
        compiler_params=small_vmem,
        name="project",
    )(inbox)
    arrived = lax.all_to_all(
        sent.reshape(experts, 4, block), "ep", 0, 0, axis_index_groups=same_core, tiled=True
    ).reshape(rows, block)
    over_tp = lax.all_to_all(
        jnp.broadcast_to(arrived, (tp, rows, block)), "tp", 0, 0, tiled=True
    )
    both = lax.all_gather(over_tp, "ep", axis_index_groups=pairs)
    stay, away = pl.pallas_call(
        expert_kernel,
        out_shape=[jax.ShapeDtypeStruct((tp, rows, block), bf16)] * 2,
        in_specs=[VMEM] * 5,
        out_specs=[VMEM] * 2,
        scratch_shapes=[pltpu.VMEM((rows, width), bf16)],
        compiler_params=pltpu.CompilerParams(vmem_limit_bytes=20 << 20),
        name="expert",
    )(both, gain, jnp.swapaxes(w_gate[0], 0, 1), jnp.swapaxes(w_up[0], 0, 1), w_down[0])
    swapped = lax.all_gather(away, "ep", axis_index_groups=pairs)
    partial = pl.pallas_call(
        pair_kernel,
        out_shape=jax.ShapeDtypeStruct((tp, rows, block), bf16),
        in_specs=[VMEM] * 2,
        out_specs=VMEM,
        compiler_params=small_vmem,
        name="pair",
    )(stay, swapped)
    pieces = lax.all_to_all(partial, "tp", 0, 0, tiled=True)
    unit_out = jnp.sum(pieces.astype(f32), axis=0).astype(bf16)
    returned = lax.all_to_all(
        unit_out.reshape(experts, 4, block), "ep", 0, 0, axis_index_groups=same_core, tiled=True
    ).reshape(rows, block)
    send, keep = pl.pallas_call(
        combine_kernel,
        out_shape=[
            jax.ShapeDtypeStruct((group_rows, block), bf16),
            jax.ShapeDtypeStruct((group_rows, block), f32),
        ],
        in_specs=[VMEM] * 3,
        out_specs=[VMEM] * 2,
        compiler_params=small_vmem,
        name="combine",
    )(returned, meta, residual)
    return pl.pallas_call(
        finish_kernel,
        out_shape=jax.ShapeDtypeStruct((group_rows, quarter), bf16),
        in_specs=[VMEM] * 2,
        out_specs=VMEM,
        compiler_params=small_vmem,
        name="finish",
    )(lax.all_gather(send, "ep", axis_index_groups=pairs), keep)


def solution(mesh):
    placed = (
        P("ep", None),
        P(),
        P(),
        P(),
        P(),
        P(),
        P(),
        P(),
        P(),
        P(),
        P(),
        P("tp", None),
        P(("ep", "tp"), None, None),
        P(("ep", "tp"), None, None),
        P(("ep", "tp")),
        P(),
        P("ep", None),
        P("ep", None),
        P("ep", None, "tp"),
        P("ep", None, "tp"),
        P("ep", "tp", None),
    )
    return jax.shard_map(
        per_device, mesh=mesh, in_specs=placed, out_specs=P("ep", "tp"), check_vma=False
    )
```

```python
import math

import jax
import jax.numpy as jnp
from jax import lax
from jax.experimental import pallas as pl
from jax.experimental.pallas import tpu as pltpu
from jax.sharding import PartitionSpec as P

HEADS = 8
NOPE = 64
ROPE = 32
VDIM = 64
KVLORA = 128

eps = 1e-06
rope_base = 10000.0
VMEM = pl.BlockSpec(memory_space=pltpu.VMEM)
HBM = pl.BlockSpec(memory_space=pltpu.HBM)
NT = (((1,), (1,)), ((), ()))
TN = (((0,), (0,)), ((), ()))
f32 = jnp.float32
bf16 = jnp.bfloat16


def dot(a, b, dims=(((1,), (0,)), ((), ()))):
    return lax.dot_general(a, b, dims, preferred_element_type=f32)


def iota(shape, dim):
    return lax.broadcasted_iota(jnp.int32, shape, dim)


def rms(values, gain):
    return values * lax.rsqrt(jnp.mean(values * values, axis=-1, keepdims=True) + eps) * gain


def turn(values, cosine, sine):
    width = values.shape[-1]
    lanes = iota(values.shape, 1) % ROPE
    ahead = pltpu.roll(values, width - ROPE // 2, 1)
    behind = pltpu.roll(values, ROPE // 2, 1)
    turned = jnp.where(lanes < ROPE // 2, -ahead, behind)
    return values * cosine + turned * sine


def angles_of(positions, width):
    lane = (iota((positions.shape[0], width), 1) % (ROPE // 2)).astype(f32)
    angle = positions * jnp.exp(lane * (-2.0 / ROPE * math.log(rope_base)))
    turns = jnp.floor(angle * (0.5 / math.pi) + 0.5)
    angle = (angle - turns * 6.28125) - turns * (2.0 * math.pi - 6.28125)
    return jnp.cos(angle), jnp.sin(angle)


def attend_kernel(
    h_lengths, h_attn_gain, h_q_gain, h_kv_gain, h_ffn_gain, h_routes, h_weights, h_hidden, h_wqd,
    h_wqn, h_wqr, h_wkv, h_wkr, h_wuk, h_rope, h_latent, h_wuv, h_wout, payload, gain_out, lengths,
    attn_gain, q_gain, kv_gain, routes, weights, hidden, wqd, wqn, wqr, wkv, wkr, wuk, rope,
    latent, wuv, sems,
):
    own = latent.shape[0]
    rows, width = hidden.shape
    tp = rows // own
    block = width // (2 * tp)
    part = h_wout.shape[0] // 2
    t = lax.axis_index("tp")
    c = lax.axis_index("ep") % 2
    moves = [
        (h_hidden, hidden), (h_attn_gain, attn_gain), (h_lengths, lengths), (h_wqd, wqd),
        (h_q_gain, q_gain), (h_wqn, wqn), (h_wqr, wqr), (h_wuk, wuk), (h_wkv, wkv), (h_wkr, wkr),
        (h_kv_gain, kv_gain), (h_rope, rope), (h_latent, latent), (h_wuv, wuv), (h_routes, routes),
        (h_weights, weights), (h_ffn_gain, gain_out),
    ]
    for j in range(2 * tp):
        column = (2 * (j % tp) + j // tp) * block
        moves.append(
            (
                h_wout.at[pl.ds(pl.multiple_of(c * part, part), part), column : column + block],
                payload.at[j, 0:part, :],
            )
        )
    copies = [pltpu.make_async_copy(src, dst, sems.at[n]) for n, (src, dst) in enumerate(moves)]
    for copy in copies:
        copy.start()

    row, col = iota((rows, rows), 0), iota((rows, rows), 1)
    pick = jnp.where(
        (iota((8, rows), 1) == t * own + iota((8, rows), 0)) & (iota((8, rows), 0) < own), 1.0, 0.0
    ).astype(bf16)
    copies[0].wait()
    own_hidden = dot(pick, hidden[...])
    copies[1].wait()
    normed = rms(own_hidden, attn_gain[...]).astype(bf16)
    copies[2].wait()
    positions = jnp.zeros((8, 1), f32)
    for s in range(own):
        positions = jnp.where(iota((8, 1), 0) == s, lengths[s].astype(f32), positions)
    cosine, sine = angles_of(positions, HEADS * ROPE)
    copies[3].wait()
    q_first = dot(normed, wqd[...])
    copies[4].wait()
    q_small = rms(q_first, q_gain[...]).astype(bf16)
    copies[5].wait()
    q_plain = dot(q_small, wqn[...])
    copies[6].wait()
    q_turned = turn(dot(q_small, wqr[...]), cosine, sine)

    def spread(values, size):
        head = iota((HEADS, values.shape[1]), 1) // size
        mask = head == iota((HEADS, values.shape[1]), 0)
        return jnp.concatenate(
            [jnp.where(mask, values[s : s + 1, :], 0.0) for s in range(own)], axis=0
        ).astype(bf16)

    def per_head(values):
        return jnp.concatenate(
            [jnp.broadcast_to(values[s : s + 1, :], (HEADS, values.shape[1])) for s in range(own)],
            axis=0,
        )

    copies[7].wait()
    q_latent = dot(spread(q_plain, NOPE), wuk[...], NT).astype(bf16)
    fold = jnp.where(
        iota((HEADS * ROPE, ROPE), 0) % ROPE == iota((HEADS * ROPE, ROPE), 1), 1.0, 0.0
    ).astype(bf16)
    q_rope = dot(spread(q_turned, ROPE), fold).astype(bf16)
    copies[8].wait()
    latent_first = dot(normed, wkv[...])
    copies[9].wait()
    plain_key = dot(normed, wkr[...], NT)
    copies[10].wait()
    new_latent = per_head(rms(latent_first, kv_gain[...]).astype(bf16).astype(f32))
    swap = jnp.concatenate([-plain_key[:, ROPE // 2 :], plain_key[:, : ROPE // 2]], axis=1)
    new_rope = per_head(
        (plain_key * cosine[:, :ROPE] + swap * sine[:, :ROPE]).astype(bf16).astype(f32)
    )
    scale = (NOPE + ROPE) ** (-0.5)
    fresh = (
        jnp.sum(q_latent.astype(f32) * new_latent, axis=1, keepdims=True)
        + jnp.sum(q_rope.astype(f32) * new_rope, axis=1, keepdims=True)
    ) * scale
    copies[11].wait()
    copies[12].wait()
    limits = per_head(positions).astype(jnp.int32)
    heads = [slice(s * HEADS, (s + 1) * HEADS) for s in range(own)]
    scores = jnp.concatenate(
        [dot(q_latent[h], latent[s], NT) + dot(q_rope[h], rope[s]) for s, h in enumerate(heads)],
        axis=0,
    )
    scores = jnp.where(iota(scores.shape, 1) < limits, scores * scale, -1e30)
    highest = jnp.maximum(jnp.max(scores, axis=1, keepdims=True), fresh)
    past = jnp.exp(scores - highest)
    now = jnp.exp(fresh - highest)
    divisor = jnp.sum(past, axis=1, keepdims=True) + now
    past = (past / divisor).astype(bf16)
    mix = jnp.concatenate([dot(past[h], latent[s]) for s, h in enumerate(heads)], axis=0)
    mix = (mix + (now / divisor).astype(bf16).astype(f32) * new_latent).astype(bf16)
    copies[13].wait()
    values = dot(mix, wuv[...])
    head = iota((HEADS, HEADS * VDIM), 1) // VDIM == iota((HEADS, HEADS * VDIM), 0)
    head_values = jnp.concatenate(
        [jnp.sum(jnp.where(head, values[h], 0.0), axis=0, keepdims=True) for h in heads], axis=0
    )

    copies[14].wait()
    copies[15].wait()
    copies[16].wait()
    r0, r1 = routes[0:1, :], routes[1:2, :]
    lane = iota((rows, 128), 1)
    meta = jnp.zeros((rows, 128), f32)
    for k, line in enumerate((r0, r1)):
        mine = jnp.sum(jnp.where(row == col, line, 0), axis=1, keepdims=True)
        hits = jnp.where(r0 == mine, 1, 0) + jnp.where(r1 == mine, 1, 0)
        slot = jnp.sum(jnp.where(col < row, hits, 0), axis=1, keepdims=True)
        meta = jnp.where(lane == k, (mine * 4 + c * 2 + slot).astype(f32), meta)
        rest = jnp.sum(jnp.where(row == col, weights[k : k + 1, :], 0.0), axis=1, keepdims=True)
        for n in range(3):
            piece = rest.astype(bf16).astype(f32)
            meta = jnp.where(lane == 2 + 3 * k + n, piece, meta)
            rest = rest - piece
    own_meta = dot(pick, meta.astype(bf16))
    section = HEADS * VDIM // tp
    parts = [head_values[:, b * section : (b + 1) * section] for b in range(tp)]
    for j in range(2 * tp):
        column = (2 * (j % tp) + j // tp) * block
        payload[j, part:, :] = jnp.concatenate(
            [*parts, own_hidden[:own, column : column + block], own_meta[:own]], axis=0
        ).astype(bf16)
    for copy in copies[17:]:
        copy.wait()


def project_kernel(inbox, sent, residual_out, meta_out):
    devices, lines, block = inbox.shape
    tp = devices // 2
    own = 4
    part = lines - own * (tp + 2)
    tails = [inbox[j, part:, :].astype(f32) for j in range(devices)]

    def section(n):
        return jnp.concatenate([tail[n * own : (n + 1) * own] for tail in tails], axis=0)

    total = jnp.zeros((devices * own, block), f32)
    for b in range(tp):
        w = jnp.concatenate([inbox[b, :part, :], inbox[tp + b, :part, :]], axis=0)
        total = total + dot(section(b).astype(bf16), w).astype(bf16).astype(f32)
    residual = section(tp) + total
    meta = section(tp + 1)
    targets = meta.astype(jnp.int32)
    lanes = iota((devices * own, sent.shape[0]), 1)
    chooser = jnp.where(
        (targets[:, 0:1] == lanes) | (targets[:, 1:2] == lanes), 1.0, 0.0
    ).astype(bf16)
    sent[...] = dot(chooser, residual.astype(bf16), TN).astype(bf16)
    residual_out[...] = residual
    meta_out[...] = meta


def expert_kernel(both, gain, wg, wu, wd, stay, away, x):
    c = lax.axis_index("ep") % 2
    cores, tp, rows, block = both.shape
    quarter = cores * block
    for part in range(2):
        size = rows // 2
        here = slice(part * size, (part + 1) * size)
        values = jnp.concatenate(
            [both[n, t, here, :] for t in range(tp) for n in range(cores)], axis=1
        ).astype(f32)
        x[here, :] = rms(values, gain[...]).astype(bf16)
    gate = dot(x[...], wg[...], NT)
    up = dot(x[...], wu[...], NT)
    inner = (gate / (1.0 + jnp.exp(-gate)) * up).astype(bf16)
    for t in range(tp):
        term = dot(inner, wd[:, t * quarter : (t + 1) * quarter])
        first, second = term[:, :block], term[:, block:]
        stay[t] = jnp.where(c == 0, first, second).astype(bf16)
        away[t] = jnp.where(c == 0, second, first).astype(bf16)


def pair_kernel(stay, swapped, out):
    partner = 1 - lax.axis_index("ep") % 2
    for t in range(stay.shape[0]):
        out[t] = (stay[t].astype(f32) + swapped[partner, t].astype(f32)).astype(bf16)


def combine_kernel(returned, meta, residual, send, keep):
    c = lax.axis_index("ep") % 2
    rows = meta.shape[0]
    group = rows // 2
    targets = meta[...].astype(jnp.int32)
    lanes = iota((rows, returned.shape[0]), 1)
    blended = jnp.zeros(residual.shape, f32)
    for k in range(2):
        chooser = jnp.where(targets[:, k : k + 1] == lanes, 1.0, 0.0).astype(bf16)
        first = 2 + 3 * k
        weight = (meta[:, first : first + 1] + meta[:, first + 1 : first + 2]) + meta[
            :, first + 2 : first + 3
        ]
        blended = blended + weight * dot(chooser, returned[...])
    total = residual[...] + blended
    send[...] = jnp.where(c == 0, total[group:], total[:group]).astype(bf16)
    keep[...] = jnp.where(c == 0, total[:group], total[group:])


def finish_kernel(swapped, keep, out):
    c = lax.axis_index("ep") % 2
    block = keep.shape[1]
    mine = keep[...]
    out[:, :block] = jnp.where(c == 0, mine, swapped[0].astype(f32)).astype(bf16)
    out[:, block:] = jnp.where(c == 0, swapped[1].astype(f32), mine).astype(bf16)


def per_device(
    hidden_in, attn_gain, w_qdown, q_gain, w_qnope, w_qrope, w_kvdown, kv_gain, w_krope, w_ukey,
    w_uvalue, w_out, cache_latent, cache_rope, lengths, ffn_gain, routes, route_weights, w_gate,
    w_up, w_down,
):
    group_rows, width = hidden_in.shape
    own = lengths.shape[0]
    tp = lax.axis_size("tp")
    experts = lax.axis_size("ep") // 2
    quarter = width // tp
    block = quarter // 2
    columns = [[(2 * k + c) * tp + t for c in range(2) for t in range(tp)] for k in range(experts)]
    same_core = [[2 * k + c for k in range(experts)] for c in range(2)]
    pairs = [[2 * k, 2 * k + 1] for k in range(experts)]

    small = [lengths, attn_gain[None], q_gain[None], kv_gain[None], ffn_gain[None], routes.T,
             route_weights.T]
    big = [hidden_in, w_qdown, w_qnope, w_qrope, w_kvdown, w_krope.T, w_ukey, cache_rope,
           cache_latent, w_uvalue]
    lines = w_out.shape[0] // 2 + own * (tp + 2)
    rows = experts * 4
    small_vmem = pltpu.CompilerParams(vmem_limit_bytes=8 << 20)
    payload, gain = pl.pallas_call(
        attend_kernel,
        out_shape=[
            jax.ShapeDtypeStruct((2 * tp, lines, block), bf16),
            jax.ShapeDtypeStruct((1, width), f32),
        ],
        in_specs=[HBM] * 18,
        out_specs=[VMEM] * 2,
        scratch_shapes=[pltpu.SMEM(lengths.shape, jnp.int32)]
        + [pltpu.VMEM(a.shape, a.dtype) for a in [*small[1:4], *small[5:], *big]]
        + [pltpu.SemaphoreType.DMA((17 + 2 * tp,))],
        compiler_params=pltpu.CompilerParams(vmem_limit_bytes=12 << 20),
        name="attend",
    )(*[pltpu.with_memory_space_constraint(a, pltpu.HBM) for a in [*small, *big, w_out]])
    inbox = lax.all_to_all(
        payload, ("ep", "tp"), 0, 0, axis_index_groups=columns, tiled=True
    )
    sent, residual, meta = pl.pallas_call(
        project_kernel,
        out_shape=[
            jax.ShapeDtypeStruct((rows, block), bf16),
            jax.ShapeDtypeStruct((2 * group_rows, block), f32),
            jax.ShapeDtypeStruct((2 * group_rows, 128), f32),
        ],
        in_specs=[VMEM],
        out_specs=[VMEM] * 3,
        compiler_params=small_vmem,
        name="project",
    )(inbox)
    arrived = lax.all_to_all(
        sent.reshape(experts, 4, block), "ep", 0, 0, axis_index_groups=same_core, tiled=True
    ).reshape(rows, block)
    over_tp = lax.all_to_all(
        jnp.broadcast_to(arrived, (tp, rows, block)), "tp", 0, 0, tiled=True
    )
    both = lax.all_gather(over_tp, "ep", axis_index_groups=pairs)
    stay, away = pl.pallas_call(
        expert_kernel,
        out_shape=[jax.ShapeDtypeStruct((tp, rows, block), bf16)] * 2,
        in_specs=[VMEM] * 5,
        out_specs=[VMEM] * 2,
        scratch_shapes=[pltpu.VMEM((rows, width), bf16)],
        compiler_params=pltpu.CompilerParams(vmem_limit_bytes=20 << 20),
        name="expert",
    )(both, gain, jnp.swapaxes(w_gate[0], 0, 1), jnp.swapaxes(w_up[0], 0, 1), w_down[0])
    swapped = lax.all_gather(away, "ep", axis_index_groups=pairs)
    partial = pl.pallas_call(
        pair_kernel,
        out_shape=jax.ShapeDtypeStruct((tp, rows, block), bf16),
        in_specs=[VMEM] * 2,
        out_specs=VMEM,
        compiler_params=small_vmem,
        name="pair",
    )(stay, swapped)
    pieces = lax.all_to_all(partial, "tp", 0, 0, tiled=True)
    unit_out = jnp.sum(pieces.astype(f32), axis=0).astype(bf16)
    returned = lax.all_to_all(
        unit_out.reshape(experts, 4, block), "ep", 0, 0, axis_index_groups=same_core, tiled=True
    ).reshape(rows, block)
    send, keep = pl.pallas_call(
        combine_kernel,
        out_shape=[
            jax.ShapeDtypeStruct((group_rows, block), bf16),
            jax.ShapeDtypeStruct((group_rows, block), f32),
        ],
        in_specs=[VMEM] * 3,
        out_specs=[VMEM] * 2,
        compiler_params=small_vmem,
        name="combine",
    )(returned, meta, residual)
    return pl.pallas_call(
        finish_kernel,
        out_shape=jax.ShapeDtypeStruct((group_rows, quarter), bf16),
        in_specs=[VMEM] * 2,
        out_specs=VMEM,
        compiler_params=small_vmem,
        name="finish",
    )(lax.all_gather(send, "ep", axis_index_groups=pairs), keep)


def solution(mesh):
    placed = (
        P("ep", None),
        P(),
        P(),
        P(),
        P(),
        P(),
        P(),
        P(),
        P(),
        P(),
        P(),
        P("tp", None),
        P(("ep", "tp"), None, None),
        P(("ep", "tp"), None, None),
        P(("ep", "tp")),
        P(),
        P("ep", None),
        P("ep", None),
        P("ep", None, "tp"),
        P("ep", None, "tp"),
        P("ep", "tp", None),
    )
    return jax.shard_map(
        per_device, mesh=mesh, in_specs=placed, out_specs=P("ep", "tp"), check_vma=False
    )
```

```python
import math

import jax
import jax.numpy as jnp
from jax import lax
from jax.experimental import pallas as pl
from jax.experimental.pallas import tpu as pltpu
from jax.sharding import PartitionSpec as P

HEADS = 8
NOPE = 64
ROPE = 32
VDIM = 64
KVLORA = 128

eps = 1e-06
rope_base = 10000.0
VMEM = pl.BlockSpec(memory_space=pltpu.VMEM)
HBM = pl.BlockSpec(memory_space=pltpu.HBM)
NT = (((1,), (1,)), ((), ()))
TN = (((0,), (0,)), ((), ()))
f32 = jnp.float32
bf16 = jnp.bfloat16


def dot(a, b, dims=(((1,), (0,)), ((), ()))):
    return lax.dot_general(a, b, dims, preferred_element_type=f32)


def iota(shape, dim):
    return lax.broadcasted_iota(jnp.int32, shape, dim)


def rms(values, gain):
    return values * lax.rsqrt(jnp.mean(values * values, axis=-1, keepdims=True) + eps) * gain


def turn(values, cosine, sine):
    width = values.shape[-1]
    lanes = iota(values.shape, 1) % ROPE
    ahead = pltpu.roll(values, width - ROPE // 2, 1)
    behind = pltpu.roll(values, ROPE // 2, 1)
    turned = jnp.where(lanes < ROPE // 2, -ahead, behind)
    return values * cosine + turned * sine


def angles_of(positions, width):
    lane = (iota((positions.shape[0], width), 1) % (ROPE // 2)).astype(f32)
    angle = positions * jnp.exp(lane * (-2.0 / ROPE * math.log(rope_base)))
    turns = jnp.floor(angle * (0.5 / math.pi) + 0.5)
    angle = (angle - turns * 6.28125) - turns * (2.0 * math.pi - 6.28125)
    return jnp.cos(angle), jnp.sin(angle)


def attend_kernel(
    h_lengths, h_attn_gain, h_q_gain, h_kv_gain, h_ffn_gain, h_routes, h_weights, h_hidden, h_wqd,
    h_wqn, h_wqr, h_wkv, h_wkr, h_wuk, h_rope, h_latent, h_wuv, payload, gain_out, lengths,
    attn_gain, q_gain, kv_gain, routes, weights, hidden, wqd, wqn, wqr, wkv, wkr, wuk, rope,
    latent, wuv, sems,
):
    own = latent.shape[0]
    rows, width = hidden.shape
    tp = rows // own
    t = lax.axis_index("tp")
    c = lax.axis_index("ep") % 2
    moves = [
        (h_hidden, hidden), (h_attn_gain, attn_gain), (h_lengths, lengths), (h_wqd, wqd),
        (h_q_gain, q_gain), (h_wqn, wqn), (h_wqr, wqr), (h_wuk, wuk), (h_wkv, wkv), (h_wkr, wkr),
        (h_kv_gain, kv_gain), (h_rope, rope), (h_latent, latent), (h_wuv, wuv), (h_routes, routes),
        (h_weights, weights), (h_ffn_gain, gain_out),
    ]
    copies = [pltpu.make_async_copy(src, dst, sems.at[n]) for n, (src, dst) in enumerate(moves)]
    for copy in copies:
        copy.start()

    row, col = iota((rows, rows), 0), iota((rows, rows), 1)
    pick = jnp.where(
        (iota((8, rows), 1) == t * own + iota((8, rows), 0)) & (iota((8, rows), 0) < own), 1.0, 0.0
    ).astype(bf16)
    copies[0].wait()
    own_hidden = dot(pick, hidden[...])
    copies[1].wait()
    normed = rms(own_hidden, attn_gain[...]).astype(bf16)
    copies[2].wait()
    positions = jnp.zeros((8, 1), f32)
    for s in range(own):
        positions = jnp.where(iota((8, 1), 0) == s, lengths[s].astype(f32), positions)
    cosine, sine = angles_of(positions, HEADS * ROPE)
    copies[3].wait()
    q_first = dot(normed, wqd[...])
    copies[4].wait()
    q_small = rms(q_first, q_gain[...]).astype(bf16)
    copies[5].wait()
    q_plain = dot(q_small, wqn[...])
    copies[6].wait()
    q_turned = turn(dot(q_small, wqr[...]), cosine, sine)

    def spread(values, size):
        head = iota((HEADS, values.shape[1]), 1) // size
        mask = head == iota((HEADS, values.shape[1]), 0)
        return jnp.concatenate(
            [jnp.where(mask, values[s : s + 1, :], 0.0) for s in range(own)], axis=0
        ).astype(bf16)

    def per_head(values):
        return jnp.concatenate(
            [jnp.broadcast_to(values[s : s + 1, :], (HEADS, values.shape[1])) for s in range(own)],
            axis=0,
        )

    copies[7].wait()
    q_latent = dot(spread(q_plain, NOPE), wuk[...], NT).astype(bf16)
    fold = jnp.where(
        iota((HEADS * ROPE, ROPE), 0) % ROPE == iota((HEADS * ROPE, ROPE), 1), 1.0, 0.0
    ).astype(bf16)
    q_rope = dot(spread(q_turned, ROPE), fold).astype(bf16)
    copies[8].wait()
    latent_first = dot(normed, wkv[...])
    copies[9].wait()
    plain_key = dot(normed, wkr[...], NT)
    copies[10].wait()
    new_latent = per_head(rms(latent_first, kv_gain[...]).astype(bf16).astype(f32))
    swap = jnp.concatenate([-plain_key[:, ROPE // 2 :], plain_key[:, : ROPE // 2]], axis=1)
    new_rope = per_head(
        (plain_key * cosine[:, :ROPE] + swap * sine[:, :ROPE]).astype(bf16).astype(f32)
    )
    scale = (NOPE + ROPE) ** (-0.5)
    fresh = (
        jnp.sum(q_latent.astype(f32) * new_latent, axis=1, keepdims=True)
        + jnp.sum(q_rope.astype(f32) * new_rope, axis=1, keepdims=True)
    ) * scale
    copies[11].wait()
    copies[12].wait()
    limits = per_head(positions).astype(jnp.int32)
    heads = [slice(s * HEADS, (s + 1) * HEADS) for s in range(own)]
    scores = jnp.concatenate(
        [dot(q_latent[h], latent[s], NT) + dot(q_rope[h], rope[s]) for s, h in enumerate(heads)],
        axis=0,
    )
    scores = jnp.where(iota(scores.shape, 1) < limits, scores * scale, -1e30)
    highest = jnp.maximum(jnp.max(scores, axis=1, keepdims=True), fresh)
    past = jnp.exp(scores - highest)
    now = jnp.exp(fresh - highest)
    divisor = jnp.sum(past, axis=1, keepdims=True) + now
    past = (past / divisor).astype(bf16)
    mix = jnp.concatenate([dot(past[h], latent[s]) for s, h in enumerate(heads)], axis=0)
    mix = (mix + (now / divisor).astype(bf16).astype(f32) * new_latent).astype(bf16)
    copies[13].wait()
    values = dot(mix, wuv[...])
    head = iota((HEADS, HEADS * VDIM), 1) // VDIM == iota((HEADS, HEADS * VDIM), 0)
    head_values = jnp.concatenate(
        [jnp.sum(jnp.where(head, values[h], 0.0), axis=0, keepdims=True) for h in heads], axis=0
    )

    copies[14].wait()
    copies[15].wait()
    copies[16].wait()
    r0, r1 = routes[0:1, :], routes[1:2, :]
    lane = iota((rows, 128), 1)
    meta = jnp.zeros((rows, 128), f32)
    for k, line in enumerate((r0, r1)):
        mine = jnp.sum(jnp.where(row == col, line, 0), axis=1, keepdims=True)
        hits = jnp.where(r0 == mine, 1, 0) + jnp.where(r1 == mine, 1, 0)
        slot = jnp.sum(jnp.where(col < row, hits, 0), axis=1, keepdims=True)
        meta = jnp.where(lane == k, (mine * 4 + c * 2 + slot).astype(f32), meta)
        rest = jnp.sum(jnp.where(row == col, weights[k : k + 1, :], 0.0), axis=1, keepdims=True)
        for n in range(3):
            piece = rest.astype(bf16).astype(f32)
            meta = jnp.where(lane == 2 + 3 * k + n, piece, meta)
            rest = rest - piece
    own_meta = dot(pick, meta.astype(bf16))
    lines = [head_values[:, n : n + 128] for n in range(0, HEADS * VDIM, 128)]
    lines += [own_hidden[:own, n : n + 128] for n in range(0, width, 128)]
    lines = jnp.concatenate([*lines, own_meta[:own]], axis=0).astype(bf16)
    for j in range(payload.shape[0]):
        payload[j] = lines


def project_kernel(inbox, w, residual, meta):
    devices, lines, block = inbox.shape
    tp, depth, width = w.shape
    own = lines // (tp + width // block + 1)
    tails = [inbox[j].astype(f32) for j in range(devices)]

    def section(n):
        return jnp.concatenate([tail[n * own : (n + 1) * own] for tail in tails], axis=0)

    meta[...] = section(tp + width // block)

    @pl.when(lax.axis_index("ep") % 2 == 0)
    def _():
        total = jnp.zeros(residual.shape, f32)
        for b in range(tp):
            total = total + dot(section(b).astype(bf16), w[b]).astype(bf16).astype(f32)
        hidden = jnp.concatenate([section(tp + n) for n in range(width // block)], axis=1)
        residual[...] = hidden + total


def select_kernel(shared, meta, sent, mine):
    c = lax.axis_index("ep") % 2
    t = lax.axis_index("tp")
    rows, width = shared.shape[1:]
    quarter = mine.shape[1]
    block = quarter // 2
    group = rows // 2
    residual = shared[0]
    half = jnp.concatenate(
        [
            jnp.where(c == 0, residual[:, n : n + block], residual[:, n + block : n + quarter])
            for n in range(0, width, quarter)
        ],
        axis=1,
    ).astype(bf16)
    targets = meta[...].astype(jnp.int32)
    lanes = iota((rows, sent.shape[0]), 1)
    chooser = jnp.where(
        (targets[:, 0:1] == lanes) | (targets[:, 1:2] == lanes), 1.0, 0.0
    ).astype(bf16)
    sent[...] = dot(chooser, half, TN).astype(bf16)
    own = jnp.where(c == 0, residual[:group], residual[group:])
    kept = own[:, :quarter]
    for n in range(1, width // quarter):
        kept = jnp.where(t == n, own[:, n * quarter : (n + 1) * quarter], kept)
    mine[...] = kept


def expert_kernel(both, gain, wg, wu, wd, stay, away, x):
    c = lax.axis_index("ep") % 2
    cores, rows, half = both.shape
    block = 128
    for part in range(2):
        here = slice(part * rows // 2, (part + 1) * rows // 2)
        values = jnp.concatenate(
            [both[n, here, m : m + block] for m in range(0, half, block) for n in range(cores)],
            axis=1,
        ).astype(f32)
        x[here, :] = rms(values, gain[...]).astype(bf16)
    gate = dot(x[...], wg[...], NT)
    up = dot(x[...], wu[...], NT)
    inner = (gate / (1.0 + jnp.exp(-gate)) * up).astype(bf16)
    for m in range(0, half, block):
        term = dot(inner, wd[:, 2 * m : 2 * m + 2 * block])
        first, second = term[:, :block], term[:, block:]
        stay[:, m : m + block] = jnp.where(c == 0, first, second).astype(bf16)
        away[:, m : m + block] = jnp.where(c == 0, second, first).astype(bf16)


def pair_kernel(stay, swapped, out):
    partner = 1 - lax.axis_index("ep") % 2
    out[...] = (stay[...].astype(f32) + swapped[partner].astype(f32)).astype(bf16)


def combine_kernel(returned, meta, out):
    rows = meta.shape[0]
    group = rows // 2
    devices, _, block = out.shape
    targets = meta[...].astype(jnp.int32)
    lanes = iota((rows, returned.shape[0]), 1)
    blended = jnp.zeros((rows, returned.shape[1]), f32)
    for k in range(2):
        chooser = jnp.where(targets[:, k : k + 1] == lanes, 1.0, 0.0).astype(bf16)
        first = 2 + 3 * k
        weight = (meta[:, first : first + 1] + meta[:, first + 1 : first + 2]) + meta[
            :, first + 2 : first + 3
        ]
        blended = blended + weight * dot(chooser, returned[...])
    tp = devices // 2
    for j in range(devices):
        g, t = j // tp, j % tp
        out[j] = blended[g * group : (g + 1) * group, t * block : (t + 1) * block]


def finish_kernel(terms, residual, out):
    devices, _, block = terms.shape
    tp = devices // 2
    for n in range(2):
        total = terms[n * tp]
        for t in range(1, tp):
            total = total + terms[n * tp + t]
        here = slice(n * block, (n + 1) * block)
        out[:, here] = (residual[:, here] + total).astype(bf16)


def per_device(
    hidden_in, attn_gain, w_qdown, q_gain, w_qnope, w_qrope, w_kvdown, kv_gain, w_krope, w_ukey,
    w_uvalue, w_out, cache_latent, cache_rope, lengths, ffn_gain, routes, route_weights, w_gate,
    w_up, w_down,
):
    group_rows, width = hidden_in.shape
    own = lengths.shape[0]
    tp = lax.axis_size("tp")
    experts = lax.axis_size("ep") // 2
    quarter = width // tp
    core = lax.axis_index("ep") % 2
    columns = [[(2 * k + c) * tp + t for c in range(2) for t in range(tp)] for k in range(experts)]
    same_core = [[2 * k + c for k in range(experts)] for c in range(2)]
    pairs = [[2 * k, 2 * k + 1] for k in range(experts)]

    small = [lengths, attn_gain[None], q_gain[None], kv_gain[None], ffn_gain[None], routes.T,
             route_weights.T]
    big = [hidden_in, w_qdown, w_qnope, w_qrope, w_kvdown, w_krope.T, w_ukey, cache_rope,
           cache_latent, w_uvalue]
    lines = own * (tp + width // 128 + 1)
    rows = experts * 4
    half = width // 2
    small_vmem = pltpu.CompilerParams(vmem_limit_bytes=8 << 20)
    payload, gain = pl.pallas_call(
        attend_kernel,
        out_shape=[
            jax.ShapeDtypeStruct((2 * tp, lines, 128), bf16),
            jax.ShapeDtypeStruct((1, width), f32),
        ],
        in_specs=[HBM] * 17,
        out_specs=[VMEM] * 2,
        scratch_shapes=[pltpu.SMEM(lengths.shape, jnp.int32)]
        + [pltpu.VMEM(a.shape, a.dtype) for a in [*small[1:4], *small[5:], *big]]
        + [pltpu.SemaphoreType.DMA((17,))],
        compiler_params=pltpu.CompilerParams(vmem_limit_bytes=12 << 20),
        name="attend",
    )(*[pltpu.with_memory_space_constraint(a, pltpu.HBM) for a in [*small, *big]])
    w_all = lax.cond(
        core == 0,
        lambda w: lax.all_to_all(jnp.broadcast_to(w, (tp, *w.shape)), "tp", 0, 0, tiled=True),
        lambda w: jnp.zeros((tp, *w.shape), w.dtype),
        w_out,
    )
    payload, w_all = lax.optimization_barrier((payload, w_all))
    inbox = lax.all_to_all(
        payload, ("ep", "tp"), 0, 0, axis_index_groups=columns, tiled=True
    )
    residual, meta = pl.pallas_call(
        project_kernel,
        out_shape=[
            jax.ShapeDtypeStruct((2 * group_rows, width), f32),
            jax.ShapeDtypeStruct((2 * group_rows, 128), f32),
        ],
        in_specs=[VMEM] * 2,
        out_specs=[VMEM] * 2,
        compiler_params=small_vmem,
        name="project",
    )(inbox, w_all)
    shared = lax.all_gather(residual, "ep", axis_index_groups=pairs)
    sent, mine = pl.pallas_call(
        select_kernel,
        out_shape=[
            jax.ShapeDtypeStruct((rows, half), bf16),
            jax.ShapeDtypeStruct((group_rows, quarter), f32),
        ],
        in_specs=[VMEM] * 2,
        out_specs=[VMEM] * 2,
        compiler_params=small_vmem,
        name="select",
    )(shared, meta)
    arrived = lax.all_to_all(
        sent.reshape(experts, 4, half), "ep", 0, 0, axis_index_groups=same_core, tiled=True
    ).reshape(rows, half)
    both = lax.all_gather(arrived, "ep", axis_index_groups=pairs)
    stay, away = pl.pallas_call(
        expert_kernel,
        out_shape=[jax.ShapeDtypeStruct((rows, half), bf16)] * 2,
        in_specs=[VMEM] * 5,
        out_specs=[VMEM] * 2,
        scratch_shapes=[pltpu.VMEM((rows, width), bf16)],
        compiler_params=pltpu.CompilerParams(vmem_limit_bytes=20 << 20),
        name="expert",
    )(both, gain, jnp.swapaxes(w_gate[0], 0, 1), jnp.swapaxes(w_up[0], 0, 1), w_down[0])
    swapped = lax.all_gather(away, "ep", axis_index_groups=pairs)
    partial = pl.pallas_call(
        pair_kernel,
        out_shape=jax.ShapeDtypeStruct((rows, half), bf16),
        in_specs=[VMEM] * 2,
        out_specs=VMEM,
        compiler_params=small_vmem,
        name="pair",
    )(stay, swapped)
    returned = lax.all_to_all(
        partial.reshape(experts, 4, half), "ep", 0, 0, axis_index_groups=same_core, tiled=True
    ).reshape(rows, half)
    terms = pl.pallas_call(
        combine_kernel,
        out_shape=jax.ShapeDtypeStruct((2 * tp, group_rows, half // tp), f32),
        in_specs=[VMEM] * 2,
        out_specs=VMEM,
        compiler_params=small_vmem,
        name="combine",
    )(returned, meta)
    terms = lax.all_to_all(terms, ("ep", "tp"), 0, 0, axis_index_groups=columns, tiled=True)
    return pl.pallas_call(
        finish_kernel,
        out_shape=jax.ShapeDtypeStruct((group_rows, quarter), bf16),
        in_specs=[VMEM] * 2,
        out_specs=VMEM,
        compiler_params=small_vmem,
        name="finish",
    )(terms, mine)


def solution(mesh):
    placed = (
        P("ep", None),
        P(),
        P(),
        P(),
        P(),
        P(),
        P(),
        P(),
        P(),
        P(),
        P(),
        P("tp", None),
        P(("ep", "tp"), None, None),
        P(("ep", "tp"), None, None),
        P(("ep", "tp")),
        P(),
        P("ep", None),
        P("ep", None),
        P("ep", None, "tp"),
        P("ep", None, "tp"),
        P("ep", "tp", None),
    )
    return jax.shard_map(
        per_device, mesh=mesh, in_specs=placed, out_specs=P("ep", "tp"), check_vma=False
    )
```

```python
import math

import jax
import jax.numpy as jnp
from jax import lax
from jax.experimental import pallas as pl
from jax.experimental.pallas import tpu as pltpu
from jax.sharding import PartitionSpec as P

HEADS = 8
NOPE = 64
ROPE = 32
VDIM = 64
KVLORA = 128

eps = 1e-06
rope_base = 10000.0
VMEM = pl.BlockSpec(memory_space=pltpu.VMEM)
HBM = pl.BlockSpec(memory_space=pltpu.HBM)
NT = (((1,), (1,)), ((), ()))
TN = (((0,), (0,)), ((), ()))
f32 = jnp.float32
bf16 = jnp.bfloat16


def dot(a, b, dims=(((1,), (0,)), ((), ()))):
    return lax.dot_general(a, b, dims, preferred_element_type=f32)


def iota(shape, dim):
    return lax.broadcasted_iota(jnp.int32, shape, dim)


def rms(values, gain):
    return values * lax.rsqrt(jnp.mean(values * values, axis=-1, keepdims=True) + eps) * gain


def turn(values, cosine, sine):
    width = values.shape[-1]
    lanes = iota(values.shape, 1) % ROPE
    ahead = pltpu.roll(values, width - ROPE // 2, 1)
    behind = pltpu.roll(values, ROPE // 2, 1)
    turned = jnp.where(lanes < ROPE // 2, -ahead, behind)
    return values * cosine + turned * sine


def angles_of(positions, width):
    lane = (iota((positions.shape[0], width), 1) % (ROPE // 2)).astype(f32)
    angle = positions * jnp.exp(lane * (-2.0 / ROPE * math.log(rope_base)))
    turns = jnp.floor(angle * (0.5 / math.pi) + 0.5)
    angle = (angle - turns * 6.28125) - turns * (2.0 * math.pi - 6.28125)
    return jnp.cos(angle), jnp.sin(angle)


def attend_kernel(
    h_lengths, h_attn_gain, h_q_gain, h_kv_gain, h_ffn_gain, h_routes, h_weights, h_hidden, h_wqd,
    h_wqn, h_wqr, h_wkv, h_wkr, h_wuk, h_rope, h_latent, h_wuv, h_wout, payload, gain_out, lengths,
    attn_gain, q_gain, kv_gain, routes, weights, hidden, wqd, wqn, wqr, wkv, wkr, wuk, rope,
    latent, wuv, sems,
):
    own = latent.shape[0]
    rows, width = hidden.shape
    tp = rows // own
    block = width // (2 * tp)
    part = h_wout.shape[0] // 2
    t = lax.axis_index("tp")
    c = lax.axis_index("ep") % 2
    moves = [
        (h_hidden, hidden), (h_attn_gain, attn_gain), (h_lengths, lengths), (h_wqd, wqd),
        (h_q_gain, q_gain), (h_wqn, wqn), (h_wqr, wqr), (h_wuk, wuk), (h_wkv, wkv), (h_wkr, wkr),
        (h_kv_gain, kv_gain), (h_rope, rope), (h_latent, latent), (h_wuv, wuv), (h_routes, routes),
        (h_weights, weights), (h_ffn_gain, gain_out),
    ]
    for j in range(2 * tp):
        column = (2 * (j % tp) + j // tp) * block
        moves.append(
            (
                h_wout.at[pl.ds(pl.multiple_of(c * part, part), part), column : column + block],
                payload.at[j, 0:part, :],
            )
        )
    copies = [pltpu.make_async_copy(src, dst, sems.at[n]) for n, (src, dst) in enumerate(moves)]
    for copy in copies:
        copy.start()

    row, col = iota((rows, rows), 0), iota((rows, rows), 1)
    pick = jnp.where(
        (iota((8, rows), 1) == t * own + iota((8, rows), 0)) & (iota((8, rows), 0) < own), 1.0, 0.0
    ).astype(bf16)
    copies[0].wait()
    own_hidden = dot(pick, hidden[...])
    copies[1].wait()
    normed = rms(own_hidden, attn_gain[...]).astype(bf16)
    copies[2].wait()
    positions = jnp.zeros((8, 1), f32)
    for s in range(own):
        positions = jnp.where(iota((8, 1), 0) == s, lengths[s].astype(f32), positions)
    cosine, sine = angles_of(positions, HEADS * ROPE)
    copies[3].wait()
    q_first = dot(normed, wqd[...])
    copies[4].wait()
    q_small = rms(q_first, q_gain[...]).astype(bf16)
    copies[5].wait()
    q_plain = dot(q_small, wqn[...])
    copies[6].wait()
    q_turned = turn(dot(q_small, wqr[...]), cosine, sine)

    def spread(values, size):
        head = iota((HEADS, values.shape[1]), 1) // size
        mask = head == iota((HEADS, values.shape[1]), 0)
        return jnp.concatenate(
            [jnp.where(mask, values[s : s + 1, :], 0.0) for s in range(own)], axis=0
        ).astype(bf16)

    def per_head(values):
        return jnp.concatenate(
            [jnp.broadcast_to(values[s : s + 1, :], (HEADS, values.shape[1])) for s in range(own)],
            axis=0,
        )

    copies[7].wait()
    q_latent = dot(spread(q_plain, NOPE), wuk[...], NT).astype(bf16)
    fold = jnp.where(
        iota((HEADS * ROPE, ROPE), 0) % ROPE == iota((HEADS * ROPE, ROPE), 1), 1.0, 0.0
    ).astype(bf16)
    q_rope = dot(spread(q_turned, ROPE), fold).astype(bf16)
    copies[8].wait()
    latent_first = dot(normed, wkv[...])
    copies[9].wait()
    plain_key = dot(normed, wkr[...], NT)
    copies[10].wait()
    new_latent = per_head(rms(latent_first, kv_gain[...]).astype(bf16).astype(f32))
    swap = jnp.concatenate([-plain_key[:, ROPE // 2 :], plain_key[:, : ROPE // 2]], axis=1)
    new_rope = per_head(
        (plain_key * cosine[:, :ROPE] + swap * sine[:, :ROPE]).astype(bf16).astype(f32)
    )
    scale = (NOPE + ROPE) ** (-0.5)
    fresh = (
        jnp.sum(q_latent.astype(f32) * new_latent, axis=1, keepdims=True)
        + jnp.sum(q_rope.astype(f32) * new_rope, axis=1, keepdims=True)
    ) * scale
    copies[11].wait()
    copies[12].wait()
    limits = per_head(positions).astype(jnp.int32)
    heads = [slice(s * HEADS, (s + 1) * HEADS) for s in range(own)]
    scores = jnp.concatenate(
        [dot(q_latent[h], latent[s], NT) + dot(q_rope[h], rope[s]) for s, h in enumerate(heads)],
        axis=0,
    )
    scores = jnp.where(iota(scores.shape, 1) < limits, scores * scale, -1e30)
    highest = jnp.maximum(jnp.max(scores, axis=1, keepdims=True), fresh)
    past = jnp.exp(scores - highest)
    now = jnp.exp(fresh - highest)
    divisor = jnp.sum(past, axis=1, keepdims=True) + now
    past = (past / divisor).astype(bf16)
    mix = jnp.concatenate([dot(past[h], latent[s]) for s, h in enumerate(heads)], axis=0)
    mix = (mix + (now / divisor).astype(bf16).astype(f32) * new_latent).astype(bf16)
    copies[13].wait()
    values = dot(mix, wuv[...])
    head = iota((HEADS, HEADS * VDIM), 1) // VDIM == iota((HEADS, HEADS * VDIM), 0)
    head_values = jnp.concatenate(
        [jnp.sum(jnp.where(head, values[h], 0.0), axis=0, keepdims=True) for h in heads], axis=0
    )

    copies[14].wait()
    copies[15].wait()
    copies[16].wait()
    r0, r1 = routes[0:1, :], routes[1:2, :]
    lane = iota((rows, 128), 1)
    meta = jnp.zeros((rows, 128), f32)
    for k, line in enumerate((r0, r1)):
        mine = jnp.sum(jnp.where(row == col, line, 0), axis=1, keepdims=True)
        hits = jnp.where(r0 == mine, 1, 0) + jnp.where(r1 == mine, 1, 0)
        slot = jnp.sum(jnp.where(col < row, hits, 0), axis=1, keepdims=True)
        meta = jnp.where(lane == k, (mine * 4 + c * 2 + slot).astype(f32), meta)
        rest = jnp.sum(jnp.where(row == col, weights[k : k + 1, :], 0.0), axis=1, keepdims=True)
        for n in range(3):
            piece = rest.astype(bf16).astype(f32)
            meta = jnp.where(lane == 2 + 3 * k + n, piece, meta)
            rest = rest - piece
    own_meta = dot(pick, meta.astype(bf16))
    section = HEADS * VDIM // tp
    parts = [head_values[:, b * section : (b + 1) * section] for b in range(tp)]
    for j in range(2 * tp):
        column = (2 * (j % tp) + j // tp) * block
        payload[j, part:, :] = jnp.concatenate(
            [*parts, own_hidden[:own, column : column + block], own_meta[:own]], axis=0
        ).astype(bf16)
    for copy in copies[17:]:
        copy.wait()


def project_kernel(inbox, sent, residual_out, meta_out):
    devices, lines, block = inbox.shape
    tp = devices // 2
    own = 4
    part = lines - own * (tp + 2)
    tails = [inbox[j, part:, :].astype(f32) for j in range(devices)]

    def section(n):
        return jnp.concatenate([tail[n * own : (n + 1) * own] for tail in tails], axis=0)

    total = jnp.zeros((devices * own, block), f32)
    for b in range(tp):
        w = jnp.concatenate([inbox[b, :part, :], inbox[tp + b, :part, :]], axis=0)
        total = total + dot(section(b).astype(bf16), w).astype(bf16).astype(f32)
    residual = section(tp) + total
    meta = section(tp + 1)
    targets = meta.astype(jnp.int32)
    lanes = iota((devices * own, sent.shape[0]), 1)
    chooser = jnp.where(
        (targets[:, 0:1] == lanes) | (targets[:, 1:2] == lanes), 1.0, 0.0
    ).astype(bf16)
    sent[...] = dot(chooser, residual.astype(bf16), TN).astype(bf16)
    residual_out[...] = residual
    meta_out[...] = meta


def expert_kernel(both, gain, residual, wg, wu, wd, stay, away, x):
    c = lax.axis_index("ep") % 2
    cores, tp, rows, block = both.shape
    size = rows // 2
    for part in range(2):
        here = slice(part * size, (part + 1) * size)
        values = jnp.concatenate(
            [both[n, t, here, :] for t in range(tp) for n in range(cores)], axis=1
        ).astype(f32)
        x[here, :] = rms(values, gain[...]).astype(bf16)
    gate = dot(x[...], wg[...], NT)
    up = dot(x[...], wu[...], NT)
    inner = (gate / (1.0 + jnp.exp(-gate)) * up).astype(bf16)
    line = iota((size, rows), 0)
    place = iota((size, rows), 1)
    first = line // 2 * 4 + line % 2
    mine = jnp.where(place == first + 2 * c, 1.0, 0.0).astype(bf16)
    other = jnp.where(place == first + 2 * (1 - c), 1.0, 0.0).astype(bf16)
    away[:size, :] = dot(dot(other, inner).astype(bf16), wd[...]).astype(bf16)
    stay[...] = dot(dot(mine, inner).astype(bf16), wd[...]).astype(bf16)
    group = residual.shape[0] // 2
    theirs = jnp.where(c == 0, residual[group:, :], residual[:group, :])
    high = theirs.astype(bf16).astype(f32)
    away[size:, :] = jnp.concatenate(
        [high, theirs - high, jnp.zeros((group, wd.shape[1] - 2 * block), f32)], axis=1
    ).astype(bf16)


def pair_kernel(stay, swapped, residual, out, kept):
    c = lax.axis_index("ep") % 2
    partner = 1 - c
    tp, rows, quarter = out.shape
    for t in range(tp):
        here = slice(t * quarter, (t + 1) * quarter)
        out[t] = (
            stay[:, here].astype(f32) + swapped[partner, :rows, here].astype(f32)
        ).astype(bf16)
    block = residual.shape[1]
    group = residual.shape[0] // 2
    extra = swapped[partner, rows:, :].astype(f32)
    theirs = extra[:, :block] + extra[:, block : 2 * block]
    own = jnp.where(c == 0, residual[:group, :], residual[group:, :])
    kept[:, :block] = jnp.where(c == 0, own, theirs)
    kept[:, block:] = jnp.where(c == 0, theirs, own)


def combine_kernel(returned, meta, residual, out):
    c = lax.axis_index("ep") % 2
    group = residual.shape[0]
    own = jnp.where(c == 0, meta[:group, :], meta[group:, :])
    targets = own.astype(jnp.int32)
    targets = targets // 4 * 2 + targets % 2
    lanes = iota((group, returned.shape[0]), 1)
    blended = jnp.zeros(residual.shape, f32)
    for k in range(2):
        chooser = jnp.where(targets[:, k : k + 1] == lanes, 1.0, 0.0).astype(bf16)
        first = 2 + 3 * k
        weight = (own[:, first : first + 1] + own[:, first + 1 : first + 2]) + own[
            :, first + 2 : first + 3
        ]
        blended = blended + weight * dot(chooser, returned[...])
    out[...] = (residual[...] + blended).astype(bf16)


def per_device(
    hidden_in, attn_gain, w_qdown, q_gain, w_qnope, w_qrope, w_kvdown, kv_gain, w_krope, w_ukey,
    w_uvalue, w_out, cache_latent, cache_rope, lengths, ffn_gain, routes, route_weights, w_gate,
    w_up, w_down,
):
    group_rows, width = hidden_in.shape
    own = lengths.shape[0]
    tp = lax.axis_size("tp")
    experts = lax.axis_size("ep") // 2
    quarter = width // tp
    block = quarter // 2
    columns = [[(2 * k + c) * tp + t for c in range(2) for t in range(tp)] for k in range(experts)]
    same_core = [[2 * k + c for k in range(experts)] for c in range(2)]
    pairs = [[2 * k, 2 * k + 1] for k in range(experts)]

    small = [lengths, attn_gain[None], q_gain[None], kv_gain[None], ffn_gain[None], routes.T,
             route_weights.T]
    big = [hidden_in, w_qdown, w_qnope, w_qrope, w_kvdown, w_krope.T, w_ukey, cache_rope,
           cache_latent, w_uvalue]
    lines = w_out.shape[0] // 2 + own * (tp + 2)
    rows = experts * 4
    small_vmem = pltpu.CompilerParams(vmem_limit_bytes=8 << 20)
    payload, gain = pl.pallas_call(
        attend_kernel,
        out_shape=[
            jax.ShapeDtypeStruct((2 * tp, lines, block), bf16),
            jax.ShapeDtypeStruct((1, width), f32),
        ],
        in_specs=[HBM] * 18,
        out_specs=[VMEM] * 2,
        scratch_shapes=[pltpu.SMEM(lengths.shape, jnp.int32)]
        + [pltpu.VMEM(a.shape, a.dtype) for a in [*small[1:4], *small[5:], *big]]
        + [pltpu.SemaphoreType.DMA((17 + 2 * tp,))],
        compiler_params=pltpu.CompilerParams(vmem_limit_bytes=12 << 20),
        name="attend",
    )(*[pltpu.with_memory_space_constraint(a, pltpu.HBM) for a in [*small, *big, w_out]])
    inbox = lax.all_to_all(
        payload, ("ep", "tp"), 0, 0, axis_index_groups=columns, tiled=True
    )
    sent, residual, meta = pl.pallas_call(
        project_kernel,
        out_shape=[
            jax.ShapeDtypeStruct((rows, block), bf16),
            jax.ShapeDtypeStruct((2 * group_rows, block), f32),
            jax.ShapeDtypeStruct((2 * group_rows, 128), f32),
        ],
        in_specs=[VMEM],
        out_specs=[VMEM] * 3,
        compiler_params=small_vmem,
        name="project",
    )(inbox)
    arrived = lax.all_to_all(
        sent.reshape(experts, 4, block), "ep", 0, 0, axis_index_groups=same_core, tiled=True
    ).reshape(rows, block)
    over_tp = lax.all_to_all(
        jnp.broadcast_to(arrived, (tp, rows, block)), "tp", 0, 0, tiled=True
    )
    both = lax.all_gather(over_tp, "ep", axis_index_groups=pairs)
    stay, away = pl.pallas_call(
        expert_kernel,
        out_shape=[
            jax.ShapeDtypeStruct((rows // 2, width), bf16),
            jax.ShapeDtypeStruct((rows // 2 + group_rows, width), bf16),
        ],
        in_specs=[VMEM] * 6,
        out_specs=[VMEM] * 2,
        scratch_shapes=[pltpu.VMEM((rows, width), bf16)],
        compiler_params=pltpu.CompilerParams(vmem_limit_bytes=20 << 20),
        name="expert",
    )(
        both, gain, residual, jnp.swapaxes(w_gate[0], 0, 1), jnp.swapaxes(w_up[0], 0, 1),
        w_down[0],
    )
    swapped = lax.all_gather(away, "ep", axis_index_groups=pairs)
    partial, kept = pl.pallas_call(
        pair_kernel,
        out_shape=[
            jax.ShapeDtypeStruct((tp, rows // 2, quarter), bf16),
            jax.ShapeDtypeStruct((group_rows, quarter), f32),
        ],
        in_specs=[VMEM] * 3,
        out_specs=[VMEM] * 2,
        compiler_params=small_vmem,
        name="pair",
    )(stay, swapped, residual)
    pieces = lax.all_to_all(partial, "tp", 0, 0, tiled=True)
    unit_out = jnp.sum(pieces.astype(f32), axis=0).astype(bf16)
    returned = lax.all_to_all(
        unit_out.reshape(experts, 2, quarter), "ep", 0, 0, axis_index_groups=same_core, tiled=True
    ).reshape(rows // 2, quarter)
    return pl.pallas_call(
        combine_kernel,
        out_shape=jax.ShapeDtypeStruct((group_rows, quarter), bf16),
        in_specs=[VMEM] * 3,
        out_specs=VMEM,
        compiler_params=small_vmem,
        name="combine",
    )(returned, meta, kept)


def solution(mesh):
    placed = (
        P("ep", None),
        P(),
        P(),
        P(),
        P(),
        P(),
        P(),
        P(),
        P(),
        P(),
        P(),
        P("tp", None),
        P(("ep", "tp"), None, None),
        P(("ep", "tp"), None, None),
        P(("ep", "tp")),
        P(),
        P("ep", None),
        P("ep", None),
        P("ep", None, "tp"),
        P("ep", None, "tp"),
        P("ep", "tp", None),
    )
    return jax.shard_map(
        per_device, mesh=mesh, in_specs=placed, out_specs=P("ep", "tp"), check_vma=False
    )
```

```python
import math

import jax
import jax.numpy as jnp
from jax import lax
from jax.experimental import pallas as pl
from jax.experimental.pallas import tpu as pltpu
from jax.sharding import PartitionSpec as P

HEADS = 8
NOPE = 64
ROPE = 32
VDIM = 64
KVLORA = 128

eps = 1e-06
rope_base = 10000.0
VMEM = pl.BlockSpec(memory_space=pltpu.VMEM)
HBM = pl.BlockSpec(memory_space=pltpu.HBM)
NT = (((1,), (1,)), ((), ()))
TN = (((0,), (0,)), ((), ()))
f32 = jnp.float32
bf16 = jnp.bfloat16


def dot(a, b, dims=(((1,), (0,)), ((), ()))):
    return lax.dot_general(a, b, dims, preferred_element_type=f32)


def iota(shape, dim):
    return lax.broadcasted_iota(jnp.int32, shape, dim)


def rms(values, gain):
    return values * lax.rsqrt(jnp.mean(values * values, axis=-1, keepdims=True) + eps) * gain


def turn(values, cosine, sine):
    width = values.shape[-1]
    lanes = iota(values.shape, 1) % ROPE
    ahead = pltpu.roll(values, width - ROPE // 2, 1)
    behind = pltpu.roll(values, ROPE // 2, 1)
    turned = jnp.where(lanes < ROPE // 2, -ahead, behind)
    return values * cosine + turned * sine


def angles_of(positions, width):
    lane = (iota((positions.shape[0], width), 1) % (ROPE // 2)).astype(f32)
    angle = positions * jnp.exp(lane * (-2.0 / ROPE * math.log(rope_base)))
    turns = jnp.floor(angle * (0.5 / math.pi) + 0.5)
    angle = (angle - turns * 6.28125) - turns * (2.0 * math.pi - 6.28125)
    return jnp.cos(angle), jnp.sin(angle)


def attend_kernel(
    h_lengths, h_attn_gain, h_q_gain, h_kv_gain, h_ffn_gain, h_routes, h_weights, h_hidden, h_wqd,
    h_wqn, h_wqr, h_wkv, h_wkr, h_wuk, h_rope, h_latent, h_wuv, h_wout, h_wg,
    h_wu, h_wd, payload, gain_out, expert, lengths,
    attn_gain, q_gain, kv_gain, routes, weights, hidden, wqd, wqn, wqr, wkv, wkr, wuk, rope,
    latent, wuv, sems,
):
    own = latent.shape[0]
    rows, width = hidden.shape
    tp = rows // own
    block = 128
    part = 2 * h_wout.shape[0]
    t = lax.axis_index("tp")
    moves = [
        (h_hidden, hidden), (h_attn_gain, attn_gain), (h_lengths, lengths), (h_wqd, wqd),
        (h_q_gain, q_gain), (h_wqn, wqn), (h_wqr, wqr), (h_wuk, wuk), (h_wkv, wkv), (h_wkr, wkr),
        (h_kv_gain, kv_gain), (h_rope, rope), (h_latent, latent), (h_wuv, wuv), (h_routes, routes),
        (h_weights, weights), (h_ffn_gain, gain_out),
    ]
    for j in range(tp):
        for n in range(2):
            column = (2 * j + n) * block
            here = slice(n * part // 2, (n + 1) * part // 2)
            moves.append((h_wout.at[:, column : column + block], payload.at[j, here, :]))
    units = h_wd.shape[0]
    for n, source in enumerate((h_wg, h_wu, h_wd)):
        moves.append((source, expert.at[n * units : (n + 1) * units, :]))
    copies = [pltpu.make_async_copy(src, dst, sems.at[n]) for n, (src, dst) in enumerate(moves)]
    for copy in copies:
        copy.start()

    row, col = iota((rows, rows), 0), iota((rows, rows), 1)
    pick = jnp.where(
        (iota((8, rows), 1) == t * own + iota((8, rows), 0)) & (iota((8, rows), 0) < own), 1.0, 0.0
    ).astype(bf16)
    copies[0].wait()
    own_hidden = dot(pick, hidden[...])
    copies[1].wait()
    normed = rms(own_hidden, attn_gain[...]).astype(bf16)
    copies[2].wait()
    positions = jnp.zeros((8, 1), f32)
    for s in range(own):
        positions = jnp.where(iota((8, 1), 0) == s, lengths[s].astype(f32), positions)
    cosine, sine = angles_of(positions, HEADS * ROPE)
    copies[3].wait()
    q_first = dot(normed, wqd[...])
    copies[4].wait()
    q_small = rms(q_first, q_gain[...]).astype(bf16)
    copies[5].wait()
    q_plain = dot(q_small, wqn[...])
    copies[6].wait()
    q_turned = turn(dot(q_small, wqr[...]), cosine, sine)

    def spread(values, size):
        head = iota((HEADS, values.shape[1]), 1) // size
        mask = head == iota((HEADS, values.shape[1]), 0)
        return jnp.concatenate(
            [jnp.where(mask, values[s : s + 1, :], 0.0) for s in range(own)], axis=0
        ).astype(bf16)

    def per_head(values):
        return jnp.concatenate(
            [jnp.broadcast_to(values[s : s + 1, :], (HEADS, values.shape[1])) for s in range(own)],
            axis=0,
        )

    copies[7].wait()
    q_latent = dot(spread(q_plain, NOPE), wuk[...], NT).astype(bf16)
    fold = jnp.where(
        iota((HEADS * ROPE, ROPE), 0) % ROPE == iota((HEADS * ROPE, ROPE), 1), 1.0, 0.0
    ).astype(bf16)
    q_rope = dot(spread(q_turned, ROPE), fold).astype(bf16)
    copies[8].wait()
    latent_first = dot(normed, wkv[...])
    copies[9].wait()
    plain_key = dot(normed, wkr[...], NT)
    copies[10].wait()
    new_latent = per_head(rms(latent_first, kv_gain[...]).astype(bf16).astype(f32))
    swap = jnp.concatenate([-plain_key[:, ROPE // 2 :], plain_key[:, : ROPE // 2]], axis=1)
    new_rope = per_head(
        (plain_key * cosine[:, :ROPE] + swap * sine[:, :ROPE]).astype(bf16).astype(f32)
    )
    scale = (NOPE + ROPE) ** (-0.5)
    fresh = (
        jnp.sum(q_latent.astype(f32) * new_latent, axis=1, keepdims=True)
        + jnp.sum(q_rope.astype(f32) * new_rope, axis=1, keepdims=True)
    ) * scale
    copies[11].wait()
    copies[12].wait()
    limits = per_head(positions).astype(jnp.int32)
    heads = [slice(s * HEADS, (s + 1) * HEADS) for s in range(own)]
    scores = jnp.concatenate(
        [dot(q_latent[h], latent[s], NT) + dot(q_rope[h], rope[s]) for s, h in enumerate(heads)],
        axis=0,
    )
    scores = jnp.where(iota(scores.shape, 1) < limits, scores * scale, -1e30)
    highest = jnp.maximum(jnp.max(scores, axis=1, keepdims=True), fresh)
    past = jnp.exp(scores - highest)
    now = jnp.exp(fresh - highest)
    divisor = jnp.sum(past, axis=1, keepdims=True) + now
    past = (past / divisor).astype(bf16)
    mix = jnp.concatenate([dot(past[h], latent[s]) for s, h in enumerate(heads)], axis=0)
    mix = (mix + (now / divisor).astype(bf16).astype(f32) * new_latent).astype(bf16)
    copies[13].wait()
    values = dot(mix, wuv[...])
    head = iota((HEADS, HEADS * VDIM), 1) // VDIM == iota((HEADS, HEADS * VDIM), 0)
    head_values = jnp.concatenate(
        [jnp.sum(jnp.where(head, values[h], 0.0), axis=0, keepdims=True) for h in heads], axis=0
    )

    copies[14].wait()
    copies[15].wait()
    copies[16].wait()
    r0, r1 = routes[0:1, :], routes[1:2, :]
    lane = iota((rows, 128), 1)
    meta = jnp.zeros((rows, 128), f32)
    for k, line in enumerate((r0, r1)):
        mine = jnp.sum(jnp.where(row == col, line, 0), axis=1, keepdims=True)
        hits = jnp.where(r0 == mine, 1, 0) + jnp.where(r1 == mine, 1, 0)
        slot = jnp.sum(jnp.where(col < row, hits, 0), axis=1, keepdims=True)
        meta = jnp.where(lane == k, (mine * 2 + slot).astype(f32), meta)
        rest = jnp.sum(jnp.where(row == col, weights[k : k + 1, :], 0.0), axis=1, keepdims=True)
        for n in range(3):
            piece = rest.astype(bf16).astype(f32)
            meta = jnp.where(lane == 2 + 3 * k + n, piece, meta)
            rest = rest - piece
    own_meta = dot(pick, meta.astype(bf16))
    parts = [head_values[:, n : n + block] for n in range(0, HEADS * VDIM, block)]
    for j in range(tp):
        column = 2 * j * block
        payload[j, part:, :] = jnp.concatenate(
            [
                *parts,
                own_hidden[:own, column : column + block],
                own_hidden[:own, column + block : column + 2 * block],
                own_meta[:own],
                jnp.zeros((own, block), f32),
            ],
            axis=0,
        ).astype(bf16)
    for copy in copies[17:]:
        copy.wait()


def project_kernel(inbox, sent, residual_out, meta_out):
    tp, lines, block = inbox.shape
    own = residual_out.shape[0] // tp
    part = lines - own * (tp + 4)
    tails = [inbox[j, part:, :].astype(f32) for j in range(tp)]

    def section(n):
        return jnp.concatenate([tail[n * own : (n + 1) * own] for tail in tails], axis=0)

    total = jnp.zeros(residual_out.shape, f32)
    for b in range(tp):
        w = jnp.concatenate([inbox[b, : part // 2, :], inbox[b, part // 2 : part, :]], axis=1)
        total = total + dot(section(b).astype(bf16), w).astype(bf16).astype(f32)
    residual = jnp.concatenate([section(tp), section(tp + 1)], axis=1) + total
    meta = section(tp + 2)
    targets = meta.astype(jnp.int32)
    lanes = iota((tp * own, sent.shape[0]), 1)
    chooser = jnp.where(
        (targets[:, 0:1] == lanes) | (targets[:, 1:2] == lanes), 1.0, 0.0
    ).astype(bf16)
    sent[...] = dot(chooser, residual.astype(bf16), TN).astype(bf16)
    residual_out[...] = residual
    meta_out[...] = meta


def expert_kernel(gathered, gain, own, h_partner, out, x, partner, sem):
    copy = pltpu.make_async_copy(h_partner, partner, sem)
    copy.start()
    tp, rows, quarter = gathered.shape
    values = jnp.concatenate([gathered[t] for t in range(tp)], axis=1).astype(f32)
    x[...] = rms(values, gain[...]).astype(bf16)
    units = own.shape[0] // 3
    inners = []
    for w in (own, partner):
        if w is partner:
            copy.wait()
        gate = dot(x[...], w[:units, :], NT)
        up = dot(x[...], w[units : 2 * units, :], NT)
        inners.append((gate / (1.0 + jnp.exp(-gate)) * up).astype(bf16))
    for t in range(tp):
        here = slice(t * quarter, (t + 1) * quarter)
        out[t] = (
            dot(inners[0], own[2 * units :, here]) + dot(inners[1], partner[2 * units :, here])
        ).astype(bf16)


def combine_kernel(returned, meta, residual, out):
    targets = meta[...].astype(jnp.int32)
    lanes = iota((residual.shape[0], returned.shape[0]), 1)
    blended = jnp.zeros(residual.shape, f32)
    for k in range(2):
        chooser = jnp.where(targets[:, k : k + 1] == lanes, 1.0, 0.0).astype(bf16)
        first = 2 + 3 * k
        weight = (meta[:, first : first + 1] + meta[:, first + 1 : first + 2]) + meta[
            :, first + 2 : first + 3
        ]
        blended = blended + weight * dot(chooser, returned[...])
    out[...] = (residual[...] + blended).astype(bf16)


def per_device(
    hidden_in, attn_gain, w_qdown, q_gain, w_qnope, w_qrope, w_kvdown, kv_gain, w_krope, w_ukey,
    w_uvalue, w_out, cache_latent, cache_rope, lengths, ffn_gain, routes, route_weights, w_gate,
    w_up, w_down,
):
    group_rows, width = hidden_in.shape
    own = lengths.shape[0]
    tp = lax.axis_size("tp")
    experts = lax.axis_size("ep") // 2
    quarter = width // tp
    same_core = [[2 * k + c for k in range(experts)] for c in range(2)]
    swap = [(i, i ^ 1) for i in range(2 * experts)]

    small = [lengths, attn_gain[None], q_gain[None], kv_gain[None], ffn_gain[None], routes.T,
             route_weights.T]
    big = [hidden_in, w_qdown, w_qnope, w_qrope, w_kvdown, w_krope.T, w_ukey, cache_rope,
           cache_latent, w_uvalue]
    lines = 2 * w_out.shape[0] + own * (tp + 4)
    rows = experts * 2
    units = w_down.shape[1]
    last = [w_out, jnp.swapaxes(w_gate[0], 0, 1), jnp.swapaxes(w_up[0], 0, 1), w_down[0]]
    small_vmem = pltpu.CompilerParams(vmem_limit_bytes=8 << 20)
    payload, gain, halves = pl.pallas_call(
        attend_kernel,
        out_shape=[
            jax.ShapeDtypeStruct((tp, lines, 128), bf16),
            jax.ShapeDtypeStruct((1, width), f32),
            jax.ShapeDtypeStruct((3 * units, width), bf16),
        ],
        in_specs=[HBM] * 21,
        out_specs=[VMEM] * 3,
        scratch_shapes=[pltpu.SMEM(lengths.shape, jnp.int32)]
        + [pltpu.VMEM(a.shape, a.dtype) for a in [*small[1:4], *small[5:], *big]]
        + [pltpu.SemaphoreType.DMA((20 + 2 * tp,))],
        compiler_params=pltpu.CompilerParams(vmem_limit_bytes=12 << 20),
        name="attend",
    )(*[pltpu.with_memory_space_constraint(a, pltpu.HBM) for a in [*small, *big, *last]])
    partner = lax.ppermute(halves, "ep", swap)
    inbox = lax.all_to_all(payload, "tp", 0, 0, tiled=True)
    sent, residual, meta = pl.pallas_call(
        project_kernel,
        out_shape=[
            jax.ShapeDtypeStruct((rows, quarter), bf16),
            jax.ShapeDtypeStruct((group_rows, quarter), f32),
            jax.ShapeDtypeStruct((group_rows, 128), f32),
        ],
        in_specs=[VMEM],
        out_specs=[VMEM] * 3,
        compiler_params=small_vmem,
        name="project",
    )(inbox)
    arrived = lax.all_to_all(
        sent.reshape(experts, 2, quarter), "ep", 0, 0, axis_index_groups=same_core, tiled=True
    ).reshape(rows, quarter)
    gathered = lax.all_to_all(
        jnp.broadcast_to(arrived, (tp, rows, quarter)), "tp", 0, 0, tiled=True
    )
    partial = pl.pallas_call(
        expert_kernel,
        out_shape=jax.ShapeDtypeStruct((tp, rows, quarter), bf16),
        in_specs=[VMEM] * 3 + [pl.BlockSpec(memory_space=pl.ANY)],
        out_specs=VMEM,
        scratch_shapes=[
            pltpu.VMEM((rows, width), bf16),
            pltpu.VMEM((3 * units, width), bf16),
            pltpu.SemaphoreType.DMA(()),
        ],
        compiler_params=pltpu.CompilerParams(vmem_limit_bytes=20 << 20),
        name="expert",
    )(gathered, gain, halves, partner)
    pieces = lax.all_to_all(partial, "tp", 0, 0, tiled=True)
    expert_out = jnp.sum(pieces.astype(f32), axis=0).astype(bf16)
    returned = lax.all_to_all(
        expert_out.reshape(experts, 2, quarter), "ep", 0, 0, axis_index_groups=same_core,
        tiled=True,
    ).reshape(rows, quarter)
    return pl.pallas_call(
        combine_kernel,
        out_shape=jax.ShapeDtypeStruct((group_rows, quarter), bf16),
        in_specs=[VMEM] * 3,
        out_specs=VMEM,
        compiler_params=small_vmem,
        name="combine",
    )(returned, meta, residual)


def solution(mesh):
    placed = (
        P("ep", None),
        P(),
        P(),
        P(),
        P(),
        P(),
        P(),
        P(),
        P(),
        P(),
        P(),
        P("tp", None),
        P(("ep", "tp"), None, None),
        P(("ep", "tp"), None, None),
        P(("ep", "tp")),
        P(),
        P("ep", None),
        P("ep", None),
        P("ep", None, "tp"),
        P("ep", None, "tp"),
        P("ep", "tp", None),
    )
    return jax.shard_map(
        per_device, mesh=mesh, in_specs=placed, out_specs=P("ep", "tp"), check_vma=False
    )
```

```python
import math

import jax
import jax.numpy as jnp
from jax import lax
from jax.experimental import pallas as pl
from jax.experimental.pallas import tpu as pltpu
from jax.sharding import PartitionSpec as P

HEADS = 8
NOPE = 64
ROPE = 32
VDIM = 64
KVLORA = 128

eps = 1e-06
rope_base = 10000.0
VMEM = pl.BlockSpec(memory_space=pltpu.VMEM)
HBM = pl.BlockSpec(memory_space=pltpu.HBM)
NT = (((1,), (1,)), ((), ()))
TN = (((0,), (0,)), ((), ()))
f32 = jnp.float32
bf16 = jnp.bfloat16


def dot(a, b, dims=(((1,), (0,)), ((), ()))):
    return lax.dot_general(a, b, dims, preferred_element_type=f32)


def iota(shape, dim):
    return lax.broadcasted_iota(jnp.int32, shape, dim)


def rms(values, gain):
    return values * lax.rsqrt(jnp.mean(values * values, axis=-1, keepdims=True) + eps) * gain


def turn(values, cosine, sine):
    width = values.shape[-1]
    lanes = iota(values.shape, 1) % ROPE
    ahead = pltpu.roll(values, width - ROPE // 2, 1)
    behind = pltpu.roll(values, ROPE // 2, 1)
    turned = jnp.where(lanes < ROPE // 2, -ahead, behind)
    return values * cosine + turned * sine


def angles_of(positions, width):
    lane = (iota((positions.shape[0], width), 1) % (ROPE // 2)).astype(f32)
    angle = positions * jnp.exp(lane * (-2.0 / ROPE * math.log(rope_base)))
    turns = jnp.floor(angle * (0.5 / math.pi) + 0.5)
    angle = (angle - turns * 6.28125) - turns * (2.0 * math.pi - 6.28125)
    return jnp.cos(angle), jnp.sin(angle)


def attend_kernel(
    h_lengths, h_attn_gain, h_q_gain, h_kv_gain, h_ffn_gain, h_routes, h_weights, h_hidden, h_wqd,
    h_wqn, h_wqr, h_wkv, h_wkr, h_wuk, h_rope, h_latent, h_wuv, h_wout, h_wg,
    h_wu, h_wd, payload, gain_out, expert, lengths,
    attn_gain, q_gain, kv_gain, routes, weights, hidden, wqd, wqn, wqr, wkv, wkr, wuk, rope,
    latent, wuv, sems,
):
    own = latent.shape[0]
    rows, width = hidden.shape
    tp = rows // own
    block = 128
    part = 2 * h_wout.shape[0]
    t = lax.axis_index("tp")
    moves = [
        (h_hidden, hidden), (h_attn_gain, attn_gain), (h_lengths, lengths), (h_wqd, wqd),
        (h_q_gain, q_gain), (h_wqn, wqn), (h_wqr, wqr), (h_wuk, wuk), (h_wkv, wkv), (h_wkr, wkr),
        (h_kv_gain, kv_gain), (h_rope, rope), (h_latent, latent), (h_wuv, wuv), (h_routes, routes),
        (h_weights, weights), (h_ffn_gain, gain_out),
    ]
    for j in range(tp):
        for n in range(2):
            column = (2 * j + n) * block
            here = slice(n * part // 2, (n + 1) * part // 2)
            moves.append((h_wout.at[:, column : column + block], payload.at[j, here, :]))
    units = h_wd.shape[0]
    for n, source in enumerate((h_wg, h_wu, h_wd)):
        moves.append((source, expert.at[n * units : (n + 1) * units, :]))
    copies = [pltpu.make_async_copy(src, dst, sems.at[n]) for n, (src, dst) in enumerate(moves)]
    for copy in copies:
        copy.start()

    row, col = iota((rows, rows), 0), iota((rows, rows), 1)
    pick = jnp.where(
        (iota((8, rows), 1) == t * own + iota((8, rows), 0)) & (iota((8, rows), 0) < own), 1.0, 0.0
    ).astype(bf16)
    copies[0].wait()
    own_hidden = dot(pick, hidden[...])
    copies[1].wait()
    normed = rms(own_hidden, attn_gain[...]).astype(bf16)
    copies[2].wait()
    positions = jnp.zeros((8, 1), f32)
    for s in range(own):
        positions = jnp.where(iota((8, 1), 0) == s, lengths[s].astype(f32), positions)
    cosine, sine = angles_of(positions, HEADS * ROPE)
    copies[3].wait()
    q_first = dot(normed, wqd[...])
    copies[4].wait()
    q_small = rms(q_first, q_gain[...]).astype(bf16)
    copies[5].wait()
    q_plain = dot(q_small, wqn[...])
    copies[6].wait()
    q_turned = turn(dot(q_small, wqr[...]), cosine, sine)

    def spread(values, size):
        head = iota((HEADS, values.shape[1]), 1) // size
        mask = head == iota((HEADS, values.shape[1]), 0)
        return jnp.concatenate(
            [jnp.where(mask, values[s : s + 1, :], 0.0) for s in range(own)], axis=0
        ).astype(bf16)

    def per_head(values):
        return jnp.concatenate(
            [jnp.broadcast_to(values[s : s + 1, :], (HEADS, values.shape[1])) for s in range(own)],
            axis=0,
        )

    copies[7].wait()
    q_latent = dot(spread(q_plain, NOPE), wuk[...], NT).astype(bf16)
    fold = jnp.where(
        iota((HEADS * ROPE, ROPE), 0) % ROPE == iota((HEADS * ROPE, ROPE), 1), 1.0, 0.0
    ).astype(bf16)
    q_rope = dot(spread(q_turned, ROPE), fold).astype(bf16)
    copies[8].wait()
    latent_first = dot(normed, wkv[...])
    copies[9].wait()
    plain_key = dot(normed, wkr[...], NT)
    copies[10].wait()
    new_latent = per_head(rms(latent_first, kv_gain[...]).astype(bf16).astype(f32))
    swap = jnp.concatenate([-plain_key[:, ROPE // 2 :], plain_key[:, : ROPE // 2]], axis=1)
    new_rope = per_head(
        (plain_key * cosine[:, :ROPE] + swap * sine[:, :ROPE]).astype(bf16).astype(f32)
    )
    scale = (NOPE + ROPE) ** (-0.5)
    fresh = (
        jnp.sum(q_latent.astype(f32) * new_latent, axis=1, keepdims=True)
        + jnp.sum(q_rope.astype(f32) * new_rope, axis=1, keepdims=True)
    ) * scale
    copies[11].wait()
    copies[12].wait()
    limits = per_head(positions).astype(jnp.int32)
    heads = [slice(s * HEADS, (s + 1) * HEADS) for s in range(own)]
    scores = jnp.concatenate(
        [dot(q_latent[h], latent[s], NT) + dot(q_rope[h], rope[s]) for s, h in enumerate(heads)],
        axis=0,
    )
    scores = jnp.where(iota(scores.shape, 1) < limits, scores * scale, -1e30)
    highest = jnp.maximum(jnp.max(scores, axis=1, keepdims=True), fresh)
    past = jnp.exp(scores - highest)
    now = jnp.exp(fresh - highest)
    divisor = jnp.sum(past, axis=1, keepdims=True) + now
    past = (past / divisor).astype(bf16)
    mix = jnp.concatenate([dot(past[h], latent[s]) for s, h in enumerate(heads)], axis=0)
    mix = (mix + (now / divisor).astype(bf16).astype(f32) * new_latent).astype(bf16)
    copies[13].wait()
    values = dot(mix, wuv[...])
    head = iota((HEADS, HEADS * VDIM), 1) // VDIM == iota((HEADS, HEADS * VDIM), 0)
    head_values = jnp.concatenate(
        [jnp.sum(jnp.where(head, values[h], 0.0), axis=0, keepdims=True) for h in heads], axis=0
    )

    copies[14].wait()
    copies[15].wait()
    copies[16].wait()
    r0, r1 = routes[0:1, :], routes[1:2, :]
    lane = iota((rows, 128), 1)
    meta = jnp.zeros((rows, 128), f32)
    for k, line in enumerate((r0, r1)):
        mine = jnp.sum(jnp.where(row == col, line, 0), axis=1, keepdims=True)
        hits = jnp.where(r0 == mine, 1, 0) + jnp.where(r1 == mine, 1, 0)
        slot = jnp.sum(jnp.where(col < row, hits, 0), axis=1, keepdims=True)
        meta = jnp.where(lane == k, (mine * 2 + slot).astype(f32), meta)
        rest = jnp.sum(jnp.where(row == col, weights[k : k + 1, :], 0.0), axis=1, keepdims=True)
        for n in range(3):
            piece = rest.astype(bf16).astype(f32)
            meta = jnp.where(lane == 2 + 3 * k + n, piece, meta)
            rest = rest - piece
    own_meta = dot(pick, meta.astype(bf16))
    parts = [head_values[:, n : n + block] for n in range(0, HEADS * VDIM, block)]
    for j in range(tp):
        column = 2 * j * block
        payload[j, part:, :] = jnp.concatenate(
            [
                *parts,
                own_hidden[:own, column : column + block],
                own_hidden[:own, column + block : column + 2 * block],
                own_meta[:own],
                jnp.zeros((own, block), f32),
            ],
            axis=0,
        ).astype(bf16)
    for copy in copies[17:]:
        copy.wait()


def project_kernel(inbox, sent, residual_out, meta_out):
    tp, lines, block = inbox.shape
    own = residual_out.shape[0] // tp
    part = lines - own * (tp + 4)
    tails = [inbox[j, part:, :].astype(f32) for j in range(tp)]

    def section(n):
        return jnp.concatenate([tail[n * own : (n + 1) * own] for tail in tails], axis=0)

    total = jnp.zeros(residual_out.shape, f32)
    for b in range(tp):
        w = jnp.concatenate([inbox[b, : part // 2, :], inbox[b, part // 2 : part, :]], axis=1)
        total = total + dot(section(b).astype(bf16), w).astype(bf16).astype(f32)
    residual = jnp.concatenate([section(tp), section(tp + 1)], axis=1) + total
    meta = section(tp + 2)
    targets = meta.astype(jnp.int32)
    lanes = iota((tp * own, sent.shape[0]), 1)
    chooser = jnp.where(
        (targets[:, 0:1] == lanes) | (targets[:, 1:2] == lanes), 1.0, 0.0
    ).astype(bf16)
    sent[...] = dot(chooser, residual.astype(bf16), TN).astype(bf16)
    residual_out[...] = residual
    meta_out[...] = meta


def expert_kernel(gathered, gain, own, h_partner, out, x, partner, total, sems):
    tp, rows, quarter = gathered.shape
    units = own.shape[0] // 3
    copies = [
        pltpu.make_async_copy(h_partner.at[here, :], partner.at[here, :], sems.at[n])
        for n, here in enumerate((slice(0, 2 * units), slice(2 * units, 3 * units)))
    ]
    for copy in copies:
        copy.start()
    values = jnp.concatenate([gathered[t] for t in range(tp)], axis=1).astype(f32)
    x[...] = rms(values, gain[...]).astype(bf16)

    def inner(w):
        gate = dot(x[...], w[:units, :], NT)
        up = dot(x[...], w[units : 2 * units, :], NT)
        return (gate / (1.0 + jnp.exp(-gate)) * up).astype(bf16)

    total[...] = dot(inner(own), own[2 * units :, :])
    copies[0].wait()
    second = inner(partner)
    copies[1].wait()
    for t in range(tp):
        here = slice(t * quarter, (t + 1) * quarter)
        out[t] = (total[:, here] + dot(second, partner[2 * units :, here])).astype(bf16)


def combine_kernel(returned, meta, residual, out):
    targets = meta[...].astype(jnp.int32)
    lanes = iota((residual.shape[0], returned.shape[0]), 1)
    blended = jnp.zeros(residual.shape, f32)
    for k in range(2):
        chooser = jnp.where(targets[:, k : k + 1] == lanes, 1.0, 0.0).astype(bf16)
        first = 2 + 3 * k
        weight = (meta[:, first : first + 1] + meta[:, first + 1 : first + 2]) + meta[
            :, first + 2 : first + 3
        ]
        blended = blended + weight * dot(chooser, returned[...])
    out[...] = (residual[...] + blended).astype(bf16)


def per_device(
    hidden_in, attn_gain, w_qdown, q_gain, w_qnope, w_qrope, w_kvdown, kv_gain, w_krope, w_ukey,
    w_uvalue, w_out, cache_latent, cache_rope, lengths, ffn_gain, routes, route_weights, w_gate,
    w_up, w_down,
):
    group_rows, width = hidden_in.shape
    own = lengths.shape[0]
    tp = lax.axis_size("tp")
    experts = lax.axis_size("ep") // 2
    quarter = width // tp
    same_core = [[2 * k + c for k in range(experts)] for c in range(2)]
    swap = [(i, i ^ 1) for i in range(2 * experts)]

    small = [lengths, attn_gain[None], q_gain[None], kv_gain[None], ffn_gain[None], routes.T,
             route_weights.T]
    big = [hidden_in, w_qdown, w_qnope, w_qrope, w_kvdown, w_krope.T, w_ukey, cache_rope,
           cache_latent, w_uvalue]
    lines = 2 * w_out.shape[0] + own * (tp + 4)
    rows = experts * 2
    units = w_down.shape[1]
    last = [w_out, jnp.swapaxes(w_gate[0], 0, 1), jnp.swapaxes(w_up[0], 0, 1), w_down[0]]
    small_vmem = pltpu.CompilerParams(vmem_limit_bytes=8 << 20)
    payload, gain, halves = pl.pallas_call(
        attend_kernel,
        out_shape=[
            jax.ShapeDtypeStruct((tp, lines, 128), bf16),
            jax.ShapeDtypeStruct((1, width), f32),
            jax.ShapeDtypeStruct((3 * units, width), bf16),
        ],
        in_specs=[HBM] * 21,
        out_specs=[VMEM] * 3,
        scratch_shapes=[pltpu.SMEM(lengths.shape, jnp.int32)]
        + [pltpu.VMEM(a.shape, a.dtype) for a in [*small[1:4], *small[5:], *big]]
        + [pltpu.SemaphoreType.DMA((20 + 2 * tp,))],
        compiler_params=pltpu.CompilerParams(vmem_limit_bytes=12 << 20),
        name="attend",
    )(*[pltpu.with_memory_space_constraint(a, pltpu.HBM) for a in [*small, *big, *last]])
    partner = lax.ppermute(halves, "ep", swap)
    inbox = lax.all_to_all(payload, "tp", 0, 0, tiled=True)
    sent, residual, meta = pl.pallas_call(
        project_kernel,
        out_shape=[
            jax.ShapeDtypeStruct((rows, quarter), bf16),
            jax.ShapeDtypeStruct((group_rows, quarter), f32),
            jax.ShapeDtypeStruct((group_rows, 128), f32),
        ],
        in_specs=[VMEM],
        out_specs=[VMEM] * 3,
        compiler_params=small_vmem,
        name="project",
    )(inbox)
    arrived = lax.all_to_all(
        sent.reshape(experts, 2, quarter), "ep", 0, 0, axis_index_groups=same_core, tiled=True
    ).reshape(rows, quarter)
    gathered = lax.all_to_all(
        jnp.broadcast_to(arrived, (tp, rows, quarter)), "tp", 0, 0, tiled=True
    )
    partial = pl.pallas_call(
        expert_kernel,
        out_shape=jax.ShapeDtypeStruct((tp, rows, quarter), bf16),
        in_specs=[VMEM] * 3 + [pl.BlockSpec(memory_space=pl.ANY)],
        out_specs=VMEM,
        scratch_shapes=[
            pltpu.VMEM((rows, width), bf16),
            pltpu.VMEM((3 * units, width), bf16),
            pltpu.VMEM((rows, width), f32),
            pltpu.SemaphoreType.DMA((2,)),
        ],
        compiler_params=pltpu.CompilerParams(vmem_limit_bytes=20 << 20),
        name="expert",
    )(gathered, gain, halves, partner)
    pieces = lax.all_to_all(partial, "tp", 0, 0, tiled=True)
    expert_out = jnp.sum(pieces.astype(f32), axis=0).astype(bf16)
    returned = lax.all_to_all(
        expert_out.reshape(experts, 2, quarter), "ep", 0, 0, axis_index_groups=same_core,
        tiled=True,
    ).reshape(rows, quarter)
    return pl.pallas_call(
        combine_kernel,
        out_shape=jax.ShapeDtypeStruct((group_rows, quarter), bf16),
        in_specs=[VMEM] * 3,
        out_specs=VMEM,
        compiler_params=small_vmem,
        name="combine",
    )(returned, meta, residual)


def solution(mesh):
    placed = (
        P("ep", None),
        P(),
        P(),
        P(),
        P(),
        P(),
        P(),
        P(),
        P(),
        P(),
        P(),
        P("tp", None),
        P(("ep", "tp"), None, None),
        P(("ep", "tp"), None, None),
        P(("ep", "tp")),
        P(),
        P("ep", None),
        P("ep", None),
        P("ep", None, "tp"),
        P("ep", None, "tp"),
        P("ep", "tp", None),
    )
    return jax.shard_map(
        per_device, mesh=mesh, in_specs=placed, out_specs=P("ep", "tp"), check_vma=False
    )
```

```python
import math

import jax
import jax.numpy as jnp
from jax import lax
from jax.experimental import pallas as pl
from jax.experimental.pallas import tpu as pltpu
from jax.sharding import PartitionSpec as P

HEADS = 8
NOPE = 64
ROPE = 32
VDIM = 64
KVLORA = 128

eps = 1e-06
rope_base = 10000.0
VMEM = pl.BlockSpec(memory_space=pltpu.VMEM)
HBM = pl.BlockSpec(memory_space=pltpu.HBM)
NT = (((1,), (1,)), ((), ()))
TN = (((0,), (0,)), ((), ()))
f32 = jnp.float32
bf16 = jnp.bfloat16


def dot(a, b, dims=(((1,), (0,)), ((), ()))):
    return lax.dot_general(a, b, dims, preferred_element_type=f32)


def iota(shape, dim):
    return lax.broadcasted_iota(jnp.int32, shape, dim)


def rms(values, gain):
    return values * lax.rsqrt(jnp.mean(values * values, axis=-1, keepdims=True) + eps) * gain


def turn(values, cosine, sine):
    width = values.shape[-1]
    lanes = iota(values.shape, 1) % ROPE
    ahead = pltpu.roll(values, width - ROPE // 2, 1)
    behind = pltpu.roll(values, ROPE // 2, 1)
    turned = jnp.where(lanes < ROPE // 2, -ahead, behind)
    return values * cosine + turned * sine


def angles_of(positions, width):
    lane = (iota((positions.shape[0], width), 1) % (ROPE // 2)).astype(f32)
    angle = positions * jnp.exp(lane * (-2.0 / ROPE * math.log(rope_base)))
    turns = jnp.floor(angle * (0.5 / math.pi) + 0.5)
    angle = (angle - turns * 6.28125) - turns * (2.0 * math.pi - 6.28125)
    return jnp.cos(angle), jnp.sin(angle)


def attend_kernel(
    h_lengths, h_attn_gain, h_q_gain, h_kv_gain, h_ffn_gain, h_routes, h_weights, h_hidden, h_wqd,
    h_wqn, h_wqr, h_wkv, h_wkr, h_wuk, h_rope, h_latent, h_wuv, h_wout, h_wg,
    h_wu, h_wd, payload, gain_out, expert, lengths,
    attn_gain, q_gain, kv_gain, routes, weights, hidden, wqd, wqn, wqr, wkv, wkr, wuk, rope,
    latent, wuv, sems,
):
    own = latent.shape[0]
    rows, width = hidden.shape
    tp = rows // own
    block = 128
    part = 2 * h_wout.shape[0]
    t = lax.axis_index("tp")
    moves = [
        (h_hidden, hidden), (h_attn_gain, attn_gain), (h_lengths, lengths), (h_wqd, wqd),
        (h_q_gain, q_gain), (h_wqn, wqn), (h_wqr, wqr), (h_wuk, wuk), (h_wkv, wkv), (h_wkr, wkr),
        (h_kv_gain, kv_gain), (h_rope, rope), (h_latent, latent), (h_wuv, wuv), (h_routes, routes),
        (h_weights, weights), (h_ffn_gain, gain_out),
    ]
    for j in range(tp):
        for n in range(2):
            column = (2 * j + n) * block
            here = slice(n * part // 2, (n + 1) * part // 2)
            moves.append((h_wout.at[:, column : column + block], payload.at[j, here, :]))
    units = h_wd.shape[0]
    for n, source in enumerate((h_wg, h_wu, h_wd)):
        moves.append((source, expert.at[n * units : (n + 1) * units, :]))
    copies = [pltpu.make_async_copy(src, dst, sems.at[n]) for n, (src, dst) in enumerate(moves)]
    for copy in copies:
        copy.start()

    row, col = iota((rows, rows), 0), iota((rows, rows), 1)
    pick = jnp.where(
        (iota((8, rows), 1) == t * own + iota((8, rows), 0)) & (iota((8, rows), 0) < own), 1.0, 0.0
    ).astype(bf16)
    copies[0].wait()
    own_hidden = dot(pick, hidden[...])
    copies[1].wait()
    normed = rms(own_hidden, attn_gain[...]).astype(bf16)
    copies[2].wait()
    positions = jnp.zeros((8, 1), f32)
    for s in range(own):
        positions = jnp.where(iota((8, 1), 0) == s, lengths[s].astype(f32), positions)
    cosine, sine = angles_of(positions, HEADS * ROPE)
    copies[3].wait()
    q_first = dot(normed, wqd[...])
    copies[4].wait()
    q_small = rms(q_first, q_gain[...]).astype(bf16)
    copies[5].wait()
    q_plain = dot(q_small, wqn[...])
    copies[6].wait()
    q_turned = turn(dot(q_small, wqr[...]), cosine, sine)

    def spread(values, size):
        head = iota((HEADS, values.shape[1]), 1) // size
        mask = head == iota((HEADS, values.shape[1]), 0)
        return jnp.concatenate(
            [jnp.where(mask, values[s : s + 1, :], 0.0) for s in range(own)], axis=0
        ).astype(bf16)

    def per_head(values):
        return jnp.concatenate(
            [jnp.broadcast_to(values[s : s + 1, :], (HEADS, values.shape[1])) for s in range(own)],
            axis=0,
        )

    copies[7].wait()
    q_latent = dot(spread(q_plain, NOPE), wuk[...], NT).astype(bf16)
    fold = jnp.where(
        iota((HEADS * ROPE, ROPE), 0) % ROPE == iota((HEADS * ROPE, ROPE), 1), 1.0, 0.0
    ).astype(bf16)
    q_rope = dot(spread(q_turned, ROPE), fold).astype(bf16)
    copies[8].wait()
    latent_first = dot(normed, wkv[...])
    copies[9].wait()
    plain_key = dot(normed, wkr[...], NT)
    copies[10].wait()
    new_latent = per_head(rms(latent_first, kv_gain[...]).astype(bf16).astype(f32))
    swap = jnp.concatenate([-plain_key[:, ROPE // 2 :], plain_key[:, : ROPE // 2]], axis=1)
    new_rope = per_head(
        (plain_key * cosine[:, :ROPE] + swap * sine[:, :ROPE]).astype(bf16).astype(f32)
    )
    scale = (NOPE + ROPE) ** (-0.5)
    fresh = (
        jnp.sum(q_latent.astype(f32) * new_latent, axis=1, keepdims=True)
        + jnp.sum(q_rope.astype(f32) * new_rope, axis=1, keepdims=True)
    ) * scale
    copies[11].wait()
    copies[12].wait()
    limits = per_head(positions).astype(jnp.int32)
    heads = [slice(s * HEADS, (s + 1) * HEADS) for s in range(own)]
    scores = jnp.concatenate(
        [dot(q_latent[h], latent[s], NT) + dot(q_rope[h], rope[s]) for s, h in enumerate(heads)],
        axis=0,
    )
    scores = jnp.where(iota(scores.shape, 1) < limits, scores * scale, -1e30)
    highest = jnp.maximum(jnp.max(scores, axis=1, keepdims=True), fresh)
    past = jnp.exp(scores - highest)
    now = jnp.exp(fresh - highest)
    divisor = jnp.sum(past, axis=1, keepdims=True) + now
    past = (past / divisor).astype(bf16)
    mix = jnp.concatenate([dot(past[h], latent[s]) for s, h in enumerate(heads)], axis=0)
    mix = (mix + (now / divisor).astype(bf16).astype(f32) * new_latent).astype(bf16)
    copies[13].wait()
    values = dot(mix, wuv[...])
    head = iota((HEADS, HEADS * VDIM), 1) // VDIM == iota((HEADS, HEADS * VDIM), 0)
    head_values = jnp.concatenate(
        [jnp.sum(jnp.where(head, values[h], 0.0), axis=0, keepdims=True) for h in heads], axis=0
    )

    copies[14].wait()
    copies[15].wait()
    copies[16].wait()
    r0, r1 = routes[0:1, :], routes[1:2, :]
    lane = iota((rows, 128), 1)
    meta = jnp.zeros((rows, 128), f32)
    for k, line in enumerate((r0, r1)):
        mine = jnp.sum(jnp.where(row == col, line, 0), axis=1, keepdims=True)
        hits = jnp.where(r0 == mine, 1, 0) + jnp.where(r1 == mine, 1, 0)
        slot = jnp.sum(jnp.where(col < row, hits, 0), axis=1, keepdims=True)
        meta = jnp.where(lane == k, (mine * 2 + slot).astype(f32), meta)
        rest = jnp.sum(jnp.where(row == col, weights[k : k + 1, :], 0.0), axis=1, keepdims=True)
        for n in range(3):
            piece = rest.astype(bf16).astype(f32)
            meta = jnp.where(lane == 2 + 3 * k + n, piece, meta)
            rest = rest - piece
    own_meta = dot(pick, meta.astype(bf16))
    parts = [head_values[:, n : n + block] for n in range(0, HEADS * VDIM, block)]
    for j in range(tp):
        column = 2 * j * block
        payload[j, part:, :] = jnp.concatenate(
            [
                *parts,
                own_hidden[:own, column : column + block],
                own_hidden[:own, column + block : column + 2 * block],
                own_meta[:own],
                jnp.zeros((own, block), f32),
            ],
            axis=0,
        ).astype(bf16)
    for copy in copies[17:]:
        copy.wait()


def project_kernel(inbox, sent, residual_out, meta_out):
    tp, lines, block = inbox.shape
    own = residual_out.shape[0] // tp
    part = lines - own * (tp + 4)
    tails = [inbox[j, part:, :].astype(f32) for j in range(tp)]

    def section(n):
        return jnp.concatenate([tail[n * own : (n + 1) * own] for tail in tails], axis=0)

    total = jnp.zeros(residual_out.shape, f32)
    for b in range(tp):
        w = jnp.concatenate([inbox[b, : part // 2, :], inbox[b, part // 2 : part, :]], axis=1)
        total = total + dot(section(b).astype(bf16), w).astype(bf16).astype(f32)
    residual = jnp.concatenate([section(tp), section(tp + 1)], axis=1) + total
    meta = section(tp + 2)
    targets = meta.astype(jnp.int32)
    lanes = iota((tp * own, sent.shape[0]), 1)
    chooser = jnp.where(
        (targets[:, 0:1] == lanes) | (targets[:, 1:2] == lanes), 1.0, 0.0
    ).astype(bf16)
    sent[...] = dot(chooser, residual.astype(bf16), TN).astype(bf16)
    residual_out[...] = residual
    meta_out[...] = meta


def expert_kernel(gathered, gain, own, h_partner, out, x, partner, total, sems):
    tp, rows, quarter = gathered.shape
    units = own.shape[0] // 3
    copies = [
        pltpu.make_async_copy(h_partner.at[here, :], partner.at[here, :], sems.at[n])
        for n, here in enumerate((slice(0, 2 * units), slice(2 * units, 3 * units)))
    ]
    for copy in copies:
        copy.start()
    values = jnp.concatenate([gathered[t] for t in range(tp)], axis=1).astype(f32)
    x[...] = rms(values, gain[...]).astype(bf16)

    def inner(w):
        gate = dot(x[...], w[:units, :], NT)
        up = dot(x[...], w[units : 2 * units, :], NT)
        return (gate / (1.0 + jnp.exp(-gate)) * up).astype(bf16)

    total[...] = dot(inner(own), own[2 * units :, :])
    copies[0].wait()
    second = inner(partner)
    copies[1].wait()
    for t in range(tp):
        here = slice(t * quarter, (t + 1) * quarter)
        out[t] = (total[:, here] + dot(second, partner[2 * units :, here])).astype(bf16)


def combine_kernel(returned, meta, residual, out):
    targets = meta[...].astype(jnp.int32)
    lanes = iota((residual.shape[0], returned.shape[0]), 1)
    blended = jnp.zeros(residual.shape, f32)
    for k in range(2):
        chooser = jnp.where(targets[:, k : k + 1] == lanes, 1.0, 0.0).astype(bf16)
        first = 2 + 3 * k
        weight = (meta[:, first : first + 1] + meta[:, first + 1 : first + 2]) + meta[
            :, first + 2 : first + 3
        ]
        blended = blended + weight * dot(chooser, returned[...])
    out[...] = (residual[...] + blended).astype(bf16)


def per_device(
    hidden_in, attn_gain, w_qdown, q_gain, w_qnope, w_qrope, w_kvdown, kv_gain, w_krope, w_ukey,
    w_uvalue, w_out, cache_latent, cache_rope, lengths, ffn_gain, routes, route_weights, w_gate,
    w_up, w_down,
):
    group_rows, width = hidden_in.shape
    own = lengths.shape[0]
    tp = lax.axis_size("tp")
    experts = lax.axis_size("ep") // 2
    quarter = width // tp
    same_core = [[2 * k + c for k in range(experts)] for c in range(2)]
    swap = [(i, i ^ 1) for i in range(2 * experts)]

    small = [lengths, attn_gain[None], q_gain[None], kv_gain[None], ffn_gain[None], routes.T,
             route_weights.T]
    big = [hidden_in, w_qdown, w_qnope, w_qrope, w_kvdown, w_krope.T, w_ukey, cache_rope,
           cache_latent, w_uvalue]
    lines = 2 * w_out.shape[0] + own * (tp + 4)
    rows = experts * 2
    units = w_down.shape[1]
    last = [w_out, jnp.swapaxes(w_gate[0], 0, 1), jnp.swapaxes(w_up[0], 0, 1), w_down[0]]
    small_vmem = pltpu.CompilerParams(vmem_limit_bytes=8 << 20)
    payload, gain, halves = pl.pallas_call(
        attend_kernel,
        out_shape=[
            jax.ShapeDtypeStruct((tp, lines, 128), bf16),
            jax.ShapeDtypeStruct((1, width), f32),
            jax.ShapeDtypeStruct((3 * units, width), bf16),
        ],
        in_specs=[HBM] * 21,
        out_specs=[VMEM] * 3,
        scratch_shapes=[pltpu.SMEM(lengths.shape, jnp.int32)]
        + [pltpu.VMEM(a.shape, a.dtype) for a in [*small[1:4], *small[5:], *big]]
        + [pltpu.SemaphoreType.DMA((20 + 2 * tp,))],
        compiler_params=pltpu.CompilerParams(vmem_limit_bytes=12 << 20),
        name="attend",
    )(*[pltpu.with_memory_space_constraint(a, pltpu.HBM) for a in [*small, *big, *last]])
    inbox = lax.all_to_all(payload, "tp", 0, 0, tiled=True)
    inbox, halves = lax.optimization_barrier((inbox, halves))
    partner = lax.ppermute(halves, "ep", swap)
    sent, residual, meta = pl.pallas_call(
        project_kernel,
        out_shape=[
            jax.ShapeDtypeStruct((rows, quarter), bf16),
            jax.ShapeDtypeStruct((group_rows, quarter), f32),
            jax.ShapeDtypeStruct((group_rows, 128), f32),
        ],
        in_specs=[VMEM],
        out_specs=[VMEM] * 3,
        compiler_params=small_vmem,
        name="project",
    )(inbox)
    arrived = lax.all_to_all(
        sent.reshape(experts, 2, quarter), "ep", 0, 0, axis_index_groups=same_core, tiled=True
    ).reshape(rows, quarter)
    gathered = lax.all_to_all(
        jnp.broadcast_to(arrived, (tp, rows, quarter)), "tp", 0, 0, tiled=True
    )
    partial = pl.pallas_call(
        expert_kernel,
        out_shape=jax.ShapeDtypeStruct((tp, rows, quarter), bf16),
        in_specs=[VMEM] * 3 + [pl.BlockSpec(memory_space=pl.ANY)],
        out_specs=VMEM,
        scratch_shapes=[
            pltpu.VMEM((rows, width), bf16),
            pltpu.VMEM((3 * units, width), bf16),
            pltpu.VMEM((rows, width), f32),
            pltpu.SemaphoreType.DMA((2,)),
        ],
        compiler_params=pltpu.CompilerParams(vmem_limit_bytes=20 << 20),
        name="expert",
    )(gathered, gain, halves, partner)
    pieces = lax.all_to_all(partial, "tp", 0, 0, tiled=True)
    expert_out = jnp.sum(pieces.astype(f32), axis=0).astype(bf16)
    returned = lax.all_to_all(
        expert_out.reshape(experts, 2, quarter), "ep", 0, 0, axis_index_groups=same_core,
        tiled=True,
    ).reshape(rows, quarter)
    return pl.pallas_call(
        combine_kernel,
        out_shape=jax.ShapeDtypeStruct((group_rows, quarter), bf16),
        in_specs=[VMEM] * 3,
        out_specs=VMEM,
        compiler_params=small_vmem,
        name="combine",
    )(returned, meta, residual)


def solution(mesh):
    placed = (
        P("ep", None),
        P(),
        P(),
        P(),
        P(),
        P(),
        P(),
        P(),
        P(),
        P(),
        P(),
        P("tp", None),
        P(("ep", "tp"), None, None),
        P(("ep", "tp"), None, None),
        P(("ep", "tp")),
        P(),
        P("ep", None),
        P("ep", None),
        P("ep", None, "tp"),
        P("ep", None, "tp"),
        P("ep", "tp", None),
    )
    return jax.shard_map(
        per_device, mesh=mesh, in_specs=placed, out_specs=P("ep", "tp"), check_vma=False
    )
```
